32 devices in a mesh: sp: 8 (over z, x), tp: 4 (over y, core).
Axes of the slice: x: 2, y: 2, z: 4, core: 2. Of those that a mesh axis runs over, the one named last changes fastest.
Arguments:
- tokens_in: bfloat16 [4096, 4096], P(('sp', 'tp')), may hold values from -64 to 64
- w_query: bfloat16 [4096, 2048], P(None, 'tp'), may hold values from -0.09375 to 0.09375
- w_key: bfloat16 [4096, 2048], P(None, 'tp'), may hold values from -0.09375 to 0.09375
- w_value: bfloat16 [4096, 2048], P(None, 'tp'), may hold values from -0.09375 to 0.09375
- w_out: bfloat16 [2048, 4096], P('tp'), may hold values from -1 to 1
Outputs:
- mixed: bfloat16 [4096, 4096], P(('sp', 'tp'))
- log_weight: float32 [32, 4096], P('tp', 'sp')
The draws below stay inside these ranges and needn't reach their ends.
All inputs are finite; a program needn't handle non-finite values.
Results may differ from the reference program's by a relative error of at most 0.019.
Values may be sent and summed in bfloat16 or wider, within the bound.
A program may use at most 128 MiB of HBM per device.

```python
import jax
import jax.numpy as jnp
from jax import lax

D = 4096
HEADS = 32
HEAD_DIM = 64
SIDE_SPAN = 64
MIDDLE_DILATION = 8
WIDEST_DILATION = 64
TOKENS = 4096
N_TP = 4


def draw_tokens_in(key, part):
    base_key = jax.random.fold_in(jax.random.fold_in(key, 11), 0)
    values = jax.random.truncated_normal(base_key, -4.0, 4.0, (TOKENS, D), jnp.float32)
    return values.astype(jnp.bfloat16)


def steps_of(own_key, extent, cuts, low, high):
    def one(dim, shards_of):
        draws = jax.random.uniform(jax.random.fold_in(jax.random.fold_in(own_key, 6), dim), (shards_of,), jnp.float32, low / len(cuts), high / len(cuts))
        return jnp.repeat(jnp.exp(draws), extent[dim] // shards_of).reshape((-1,) + (1,) * (len(extent) - dim - 1))

    gain = one(*cuts[0])
    for cut in cuts[1:]:
        gain = gain * one(*cut)
    return gain


def gaussian(key, dims, scale, bound, shards=(), kind=jnp.bfloat16):
    entries = scale * jax.random.normal(key, dims, jnp.float32)
    if shards:
        entries = entries * steps_of(key, dims, shards, -0.22, 0.18)
    return jnp.clip(entries, -bound, bound).astype(kind)


def setup_inputs(seed: int = 0) -> dict:
    arg_keys = jax.random.split(jax.random.key(seed), 6)
    tokens_in = draw_tokens_in(jax.random.fold_in(arg_keys[5], 71), 0)
    w_query = gaussian(arg_keys[1], (D, HEADS * HEAD_DIM), D ** -0.5, 0.09375, ((1, 4),))
    w_key = gaussian(arg_keys[2], (D, HEADS * HEAD_DIM), D ** -0.5, 0.09375, ((1, 4),))
    w_value = gaussian(arg_keys[3], (D, HEADS * HEAD_DIM), D ** -0.5, 0.09375, ((1, 4),))
    w_out = gaussian(arg_keys[4], (HEADS * HEAD_DIM, D), HEADS ** -0.5, 1.0, ((0, 4),))
    return {"tokens_in": tokens_in, "w_query": w_query, "w_key": w_key, "w_value": w_value, "w_out": w_out}


ROTARY_BASE = 500000.0
NEGATIVE = -1e30


def rotate(block, positions):
    half_size = block.shape[-1] // 2
    freq = 1.0 / (ROTARY_BASE ** (jnp.arange(half_size, dtype=jnp.float32) / half_size))
    angle = positions[:, None] * freq[None, :]
    cosine = jnp.cos(angle)[:, None, :]
    sine = jnp.sin(angle)[:, None, :]
    front = block[..., :half_size]
    back = block[..., half_size:]
    return jnp.concatenate([front * cosine - back * sine, back * cosine + front * sine], axis=-1)


def pattern_attend(query, keys, values, lead_rows, dilation_step, low_row, high_row):
    rows_total, head_count, head_size = query.shape
    class_len = rows_total // dilation_step
    first_class = lead_rows // dilation_step - SIDE_SPAN
    class_q = query.reshape(class_len, dilation_step, head_count, head_size)
    class_k = keys.reshape(keys.shape[0] // dilation_step, dilation_step, head_count, head_size)
    class_v = values.reshape(values.shape[0] // dilation_step, dilation_step, head_count, head_size)
    sub_k = class_k[first_class:first_class + class_len + 2 * SIDE_SPAN]
    sub_v = class_v[first_class:first_class + class_len + 2 * SIDE_SPAN]
    if class_len <= SIDE_SPAN:
        block_len = class_len
        block_count = 1
        win_k = sub_k[None]
        win_v = sub_v[None]
        blocks_q = class_q[None]
    else:
        block_len = SIDE_SPAN
        block_count = class_len // SIDE_SPAN
        part_k = sub_k.reshape(block_count + 2, SIDE_SPAN, dilation_step, head_count, head_size)
        part_v = sub_v.reshape(block_count + 2, SIDE_SPAN, dilation_step, head_count, head_size)
        win_k = jnp.concatenate([part_k[:-2], part_k[1:-1], part_k[2:]], axis=1)
        win_v = jnp.concatenate([part_v[:-2], part_v[1:-1], part_v[2:]], axis=1)
        blocks_q = class_q.reshape(block_count, SIDE_SPAN, dilation_step, head_count, head_size)
    width = block_len + 2 * SIDE_SPAN
    scores = jnp.einsum('nasht,nksht->nshak', blocks_q, win_k, preferred_element_type=jnp.float32)
    scores = scores * (head_size ** -0.5)
    q_index = jnp.arange(block_len, dtype=jnp.int32)
    k_index = jnp.arange(width, dtype=jnp.int32)
    b_index = jnp.arange(block_count, dtype=jnp.int32)
    s_index = jnp.arange(dilation_step, dtype=jnp.int32)
    in_band = jnp.abs(k_index[None, :] - SIDE_SPAN - q_index[:, None]) <= SIDE_SPAN
    key_position = ((first_class + b_index[:, None] * block_len + k_index[None, :]) * dilation_step)[:, None, :] + s_index[None, :, None]
    is_valid = (key_position >= low_row) & (key_position < high_row)
    keep_mask = in_band[None, None, None] & is_valid[:, :, None, None, :]
    scores = jnp.where(keep_mask, scores, NEGATIVE)
    maxima = jnp.max(scores, axis=-1, keepdims=True)
    expo = jnp.exp(scores - maxima)
    totals = jnp.sum(expo, axis=-1)
    numerator = jnp.einsum('nshak,nksht->nasht', expo.astype(jnp.bfloat16), win_v, preferred_element_type=jnp.float32)
    totals_t = jnp.transpose(totals, (0, 3, 1, 2))
    result = (numerator / totals_t[..., None]).astype(jnp.bfloat16).reshape(rows_total, head_count, head_size)
    log_sum = jnp.transpose(maxima[..., 0] + jnp.log(totals), (0, 3, 1, 2)).reshape(rows_total, head_count)
    return result, log_sum


def combine(results):
    sums = jnp.stack([item[1] for item in results], axis=0)
    peak = jnp.max(sums, axis=0)
    share = jnp.exp(sums - peak[None])
    weight_sum = share[0] + share[1] + share[2]
    accum = share[0][..., None] * results[0][0].astype(jnp.float32)
    accum = accum + share[1][..., None] * results[1][0].astype(jnp.float32)
    accum = accum + share[2][..., None] * results[2][0].astype(jnp.float32)
    attended = (accum / weight_sum[..., None]).astype(jnp.bfloat16)
    return attended, peak + jnp.log(weight_sum)


def reference(tokens_in, w_query, w_key, w_value, w_out):
    positions = jnp.arange(TOKENS, dtype=jnp.float32)
    shape3 = (TOKENS, HEADS, HEAD_DIM)
    query = rotate(jnp.dot(tokens_in, w_query, preferred_element_type=jnp.float32).reshape(shape3), positions).astype(jnp.bfloat16)
    key = rotate(jnp.dot(tokens_in, w_key, preferred_element_type=jnp.float32).reshape(shape3), positions).astype(jnp.bfloat16)
    value = jnp.dot(tokens_in, w_value, preferred_element_type=jnp.float32).astype(jnp.bfloat16).reshape(shape3)
    query_h = jnp.transpose(query, (1, 0, 2))[:, :, None, :]
    key_h = jnp.transpose(key, (1, 0, 2))[:, :, None, :]
    value_h = jnp.transpose(value, (1, 0, 2))[:, :, None, :]

    def one_head(items):
        head_q, head_k, head_v = items
        results = []
        for dilation_step in (1, MIDDLE_DILATION, WIDEST_DILATION):
            border_extent = SIDE_SPAN * dilation_step
            pad_k = jnp.pad(head_k, ((border_extent, border_extent), (0, 0), (0, 0)))
            pad_v = jnp.pad(head_v, ((border_extent, border_extent), (0, 0), (0, 0)))
            results.append(pattern_attend(head_q, pad_k, pad_v, border_extent, dilation_step, border_extent, border_extent + TOKENS))
        attended, log_sum = combine(results)
        return attended[:, 0, :], log_sum[:, 0]

    attended_h, log_weight = lax.map(one_head, (query_h, key_h, value_h))
    attended = jnp.transpose(attended_h, (1, 0, 2)).reshape(TOKENS, HEADS * HEAD_DIM)
    group_cols = HEADS * HEAD_DIM // N_TP
    total = jnp.zeros((TOKENS, D), jnp.float32)
    for group in range(N_TP):
        part = jnp.dot(attended[:, group * group_cols:(group + 1) * group_cols],
                       w_out[group * group_cols:(group + 1) * group_cols], preferred_element_type=jnp.float32)
        rounded = lax.optimization_barrier(part.astype(jnp.bfloat16))
        total = total + rounded.astype(jnp.float32)
    return total.astype(jnp.bfloat16), log_weight
```

```python
import functools

import jax
import jax.numpy as jnp
import numpy as np
from jax import lax
from jax.experimental import pallas as pl
from jax.experimental.pallas import tpu as pltpu
from jax.sharding import PartitionSpec as P

HEAD_DIM = 64
SIDE_SPAN = 64
MIDDLE_DILATION = 8
WIDEST_DILATION = 64


ROTARY_BASE = 500000.0
NEGATIVE = -1e30


def shifted(block, axis, distance):
    devices = range(lax.axis_size(axis))
    route = [(i - distance, i) for i in devices if i - distance in devices]
    return lax.ppermute(block, axis, route)


def rotate(block, positions):
    half_size = block.shape[-1] // 2
    freq = 1.0 / ROTARY_BASE ** (jnp.arange(half_size, dtype=jnp.float32) / half_size)
    angle = positions[:, None] * freq[None, :]
    cosine = jnp.cos(angle)[:, None, :]
    sine = jnp.sin(angle)[:, None, :]
    front = block[..., :half_size]
    back = block[..., half_size:]
    return jnp.concatenate([front * cosine - back * sine, back * cosine + front * sine], axis=-1)


def pattern_attend(query, keys, values, lead_rows, dilation_step, low_row, high_row):
    rows_total, head_count, head_size = query.shape
    class_len = rows_total // dilation_step
    first_class = lead_rows // dilation_step - SIDE_SPAN
    class_q = query.reshape(class_len, dilation_step, head_count, head_size)
    class_k = keys.reshape(keys.shape[0] // dilation_step, dilation_step, head_count, head_size)
    class_v = values.reshape(values.shape[0] // dilation_step, dilation_step, head_count, head_size)
    sub_k = class_k[first_class : first_class + class_len + 2 * SIDE_SPAN]
    sub_v = class_v[first_class : first_class + class_len + 2 * SIDE_SPAN]
    if class_len <= SIDE_SPAN:
        block_len = class_len
        block_count = 1
        win_k = sub_k[None]
        win_v = sub_v[None]
        blocks_q = class_q[None]
    else:
        block_len = SIDE_SPAN
        block_count = class_len // SIDE_SPAN
        part_k = sub_k.reshape(block_count + 2, SIDE_SPAN, dilation_step, head_count, head_size)
        part_v = sub_v.reshape(block_count + 2, SIDE_SPAN, dilation_step, head_count, head_size)
        win_k = jnp.concatenate([part_k[:-2], part_k[1:-1], part_k[2:]], axis=1)
        win_v = jnp.concatenate([part_v[:-2], part_v[1:-1], part_v[2:]], axis=1)
        blocks_q = class_q.reshape(block_count, SIDE_SPAN, dilation_step, head_count, head_size)
    width = block_len + 2 * SIDE_SPAN
    scores = jnp.einsum("nasht,nksht->nshak", blocks_q, win_k, preferred_element_type=jnp.float32)
    scores = scores * head_size ** (-0.5)
    q_index = jnp.arange(block_len, dtype=jnp.int32)
    k_index = jnp.arange(width, dtype=jnp.int32)
    b_index = jnp.arange(block_count, dtype=jnp.int32)
    s_index = jnp.arange(dilation_step, dtype=jnp.int32)
    in_band = jnp.abs(k_index[None, :] - SIDE_SPAN - q_index[:, None]) <= SIDE_SPAN
    key_position = (
        (first_class + b_index[:, None] * block_len + k_index[None, :]) * dilation_step
    )[:, None, :] + s_index[None, :, None]
    is_valid = (key_position >= low_row) & (key_position < high_row)
    keep_mask = in_band[None, None, None] & is_valid[:, :, None, None, :]
    scores = jnp.where(keep_mask, scores, NEGATIVE)
    maxima = jnp.max(scores, axis=-1, keepdims=True)
    expo = jnp.exp(scores - maxima)
    totals = jnp.sum(expo, axis=-1)
    numerator = jnp.einsum(
        "nshak,nksht->nasht", expo.astype(jnp.bfloat16), win_v, preferred_element_type=jnp.float32
    )
    totals_t = jnp.transpose(totals, (0, 3, 1, 2))
    result = (
        (numerator / totals_t[..., None])
        .astype(jnp.bfloat16)
        .reshape(rows_total, head_count, head_size)
    )
    log_sum = jnp.transpose(maxima[..., 0] + jnp.log(totals), (0, 3, 1, 2)).reshape(
        rows_total, head_count
    )
    return (result, log_sum)


def combine(results):
    sums = jnp.stack([item[1] for item in results], axis=0)
    peak = jnp.max(sums, axis=0)
    share = jnp.exp(sums - peak[None])
    weight_sum = share[0] + share[1] + share[2]
    accum = share[0][..., None] * results[0][0].astype(jnp.float32)
    accum = accum + share[1][..., None] * results[1][0].astype(jnp.float32)
    accum = accum + share[2][..., None] * results[2][0].astype(jnp.float32)
    attended = (accum / weight_sum[..., None]).astype(jnp.bfloat16)
    return (attended, peak + jnp.log(weight_sum))


def per_device(tokens_in, w_query, w_key, w_value, w_out):
    col_count = w_query.shape[1]
    head_count = col_count // HEAD_DIM
    piece = lax.all_gather(tokens_in, "tp", axis=0, tiled=True)
    projected = jnp.concatenate(
        [
            jnp.dot(piece, w_query, preferred_element_type=jnp.float32),
            jnp.dot(piece, w_key, preferred_element_type=jnp.float32),
            jnp.dot(piece, w_value, preferred_element_type=jnp.float32),
        ],
        axis=1,
    )
    rows_total = projected.shape[0]
    sp_size = lax.axis_size("sp")
    sp_place = lax.axis_index("sp")
    positions = (sp_place * rows_total + jnp.arange(rows_total, dtype=jnp.int32)).astype(
        jnp.float32
    )
    shape3 = (rows_total, head_count, HEAD_DIM)
    query = rotate(projected[:, :col_count].reshape(shape3), positions).astype(jnp.bfloat16)
    keys = rotate(projected[:, col_count : 2 * col_count].reshape(shape3), positions).astype(
        jnp.bfloat16
    )
    values = projected[:, 2 * col_count :].astype(jnp.bfloat16).reshape(shape3)
    per_device_span = -(-(SIDE_SPAN * MIDDLE_DILATION) // rows_total)
    earlier_k = []
    earlier_v = []
    before_k, before_v = shifted((keys, values), "sp", 1)
    after_k, after_v = shifted((keys, values), "sp", -1)
    earlier_k.insert(0, before_k)
    earlier_v.insert(0, before_v)
    later_k = [after_k]
    later_v = [after_v]
    key_buf = jnp.concatenate(earlier_k + [keys] + later_k, axis=0)
    value_buf = jnp.concatenate(earlier_v + [values] + later_v, axis=0)
    lead_rows = per_device_span * rows_total
    low_row = lead_rows - sp_place * rows_total
    key_buf, value_buf, lead_rows, low_row, high_row = (
        key_buf,
        value_buf,
        lead_rows,
        low_row,
        low_row + sp_size * rows_total,
    )
    results = [
        pattern_attend(query, key_buf, value_buf, lead_rows, dilation_step, low_row, high_row)
        for dilation_step in (1, MIDDLE_DILATION)
    ]
    class_stride = WIDEST_DILATION // sp_size
    border_extent = SIDE_SPAN * class_stride
    class_shape = (rows_total // sp_size, sp_size, head_count, HEAD_DIM)
    parts = (
        lax.all_to_all(query.reshape(class_shape), "sp", split_axis=1, concat_axis=0, tiled=True),
        lax.all_to_all(keys.reshape(class_shape), "sp", split_axis=1, concat_axis=0, tiled=True),
        lax.all_to_all(values.reshape(class_shape), "sp", split_axis=1, concat_axis=0, tiled=True),
    )
    item_heads = parts[0].shape[2]
    flat = [item.reshape(rows_total, item_heads, HEAD_DIM) for item in parts]
    pad_k = jnp.pad(flat[1], ((border_extent, border_extent), (0, 0), (0, 0)))
    pad_v = jnp.pad(flat[2], ((border_extent, border_extent), (0, 0), (0, 0)))
    result, log_sum = pattern_attend(
        flat[0],
        pad_k,
        pad_v,
        border_extent,
        class_stride,
        border_extent,
        border_extent + rows_total,
    )
    result_back = lax.all_to_all(
        result.reshape(rows_total, 1, item_heads, HEAD_DIM),
        "sp",
        split_axis=0,
        concat_axis=1,
        tiled=True,
    )
    sum_back = lax.all_to_all(
        log_sum.reshape(rows_total, 1, item_heads), "sp", split_axis=0, concat_axis=1, tiled=True
    )
    results.append((result_back.reshape(shape3), sum_back.reshape(rows_total, head_count)))
    attended, log_weight = combine(results)
    flat_out = attended.reshape(rows_total, col_count)
    mixed = lax.psum_scatter(
        jnp.dot(flat_out, w_out, preferred_element_type=jnp.float32).astype(jnp.bfloat16),
        "tp",
        scatter_dimension=0,
        tiled=True,
    )
    return (mixed, jnp.transpose(log_weight, (1, 0)))


MESH_ID = pl.DeviceIdType.MESH
PAIR = 2 * HEAD_DIM
ROW_BLOCK = 128
SPLITS = 2
OUT_SPLITS = 4
SEGMENTS = 4
K, V, Q = 0, 1, 2
UNITS = ((0, (K, V)), (1, (K, V)), (2, (K, V, Q)), (0, (Q,)), (3, (K, V)), (3, (Q,)), (1, (Q,)))


def class_kernel(
    sp_size, tp_size, col_count,
    x_hbm, wq_hbm, wk_hbm, wv_hbm, wo_hbm, table_hbm,
    out_ref, logw_ref,
    x_all, w_all, wo, table, cos_t, sin_t, q_c, kv_ext, pf, cls_send, cls_recv,
    bias_near, bias_class, o_near, lse_near, cls_o, cls_lse, lse_out, ret, ret_lse, ret_f, lse_f, logw_far,
    att, part_out, part_in, cross_out, cross_in, keep_b, keep_d, own_out, own_in,
    load_sem, own_send, own_recv, far_send, far_recv, fwd_send, fwd_recv,
    a2a_send, a2a_recv, halo_send, halo_recv, back_send, back_recv, lback_send, lback_recv,
    ex_send, ex_recv, cr_send, cr_recv, ox_send, ox_recv,
):
    sp = lax.axis_index("sp")
    tp = lax.axis_index("tp")
    chip = tp // 2
    core = tp % 2
    partner = chip * 2 + (1 - core)
    far_same = (1 - chip) * 2 + core
    far_other = (1 - chip) * 2 + (1 - core)
    shard = x_hbm.shape[0]
    rows = shard * tp_size
    piece = shard // SPLITS
    group_count = col_count // PAIR
    head_count = col_count // HEAD_DIM
    share = shard // sp_size
    f32, bf16 = jnp.float32, jnp.bfloat16

    offsets = sorted(range(1, sp_size), key=lambda off: (abs(off - sp_size // 2), off))

    spans = (
        ((tp, 0, shard),),
        ((partner, 0, shard),),
        ((far_same, 0, piece), (far_other, 0, piece)),
        ((far_same, piece, piece), (far_other, piece, piece)),
    )

    def row_of(s, a, c):
        return pl.multiple_of(s * shard + a, c)

    load_table = pltpu.make_async_copy(table_hbm, table, load_sem.at[0])
    load_x = pltpu.make_async_copy(x_hbm, x_all.at[tp], load_sem.at[1])
    load_w = [
        pltpu.make_async_copy(w, w_all.at[n], load_sem.at[2 + n])
        for n, w in enumerate((wk_hbm, wv_hbm, wq_hbm))
    ]
    load_out = pltpu.make_async_copy(wo_hbm, wo, load_sem.at[5])
    load_x.start()
    load_table.start()
    for item in load_w:
        item.start()

    barrier = pltpu.get_barrier_semaphore()
    pl.semaphore_signal(barrier, inc=1, device_id={"tp": partner}, device_id_type=MESH_ID)
    pl.semaphore_signal(barrier, inc=1, device_id={"tp": far_same}, device_id_type=MESH_ID)
    for off in offsets:
        pl.semaphore_signal(
            barrier, inc=1, device_id={"sp": (sp + off) % sp_size}, device_id_type=MESH_ID
        )
    pl.semaphore_wait(barrier, 2 + (sp_size - 1))

    def remote(src, dst, send, recv, **where):
        return pltpu.make_async_remote_copy(
            src_ref=src, dst_ref=dst, send_sem=send, recv_sem=recv,
            device_id=where, device_id_type=MESH_ID,
        )

    waits = []

    def launch(item):
        item.start()
        waits.append(item)
        return item

    far = []
    for k in range(SPLITS):
        span = pl.ds(k * piece, piece)
        far.append(
            launch(
                remote(
                    x_hbm.at[span], x_all.at[tp, span], far_send.at[k], far_recv.at[k], tp=far_same
                )
            )
        )
    own = launch(remote(x_hbm, x_all.at[tp], own_send.at[0], own_recv.at[0], tp=partner))
    load_out.start()

    lane = lax.broadcasted_iota(jnp.int32, (1, PAIR), 1)
    front = lane % HEAD_DIM < HEAD_DIM // 2
    first_head = lane < HEAD_DIM
    sign = jnp.where(front, -1.0, 1.0).astype(f32)
    load_table.wait()
    base_cos = table[0, pl.ds(rows + sp, 1), :]
    base_sin = table[1, pl.ds(rows + sp, 1), :]
    for r0 in range(0, rows, ROW_BLOCK):
        lc = table[0, r0 : r0 + ROW_BLOCK]
        ls = table[1, r0 : r0 + ROW_BLOCK]
        cos_t[r0 : r0 + ROW_BLOCK] = lc * base_cos - ls * base_sin
        sin_t[r0 : r0 + ROW_BLOCK] = (ls * base_cos + lc * base_sin) * sign

    window = ROW_BLOCK + 2 * SIDE_SPAN
    mid_step = MIDDLE_DILATION // sp_size
    wide_step = WIDEST_DILATION // sp_size
    per_source = rows // sp_size
    half_share = share // 2

    def place_of(seg, index):
        source = index // share
        j = index % share
        if seg < 2:
            inner = spans[seg][0][0] * share + j
        else:
            inner = jnp.where(
                j < half_share,
                far_same * share + (seg - 2) * half_share + j,
                far_other * share + (seg - 3) * half_share + j,
            )
        return source * per_source + inner

    def build_bias():
        near_i = lax.broadcasted_iota(jnp.int32, (ROW_BLOCK, window), 0)
        near_j = lax.broadcasted_iota(jnp.int32, (ROW_BLOCK, window), 1)
        near_band = jnp.abs(near_j - SIDE_SPAN - near_i) <= SIDE_SPAN
        for r0 in range(0, rows, ROW_BLOCK):
            key_pos = sp * rows + r0 + near_j - SIDE_SPAN
            good = near_band & (key_pos >= 0) & (key_pos < sp_size * rows)
            bias_near[r0 : r0 + ROW_BLOCK] = jnp.where(good, 0.0, NEGATIVE)
        for a in range(SEGMENTS):
            q_place = place_of(a, lax.broadcasted_iota(jnp.int32, (ROW_BLOCK, 1), 0))
            for b in range(SEGMENTS):
                k_place = place_of(b, lax.broadcasted_iota(jnp.int32, (1, ROW_BLOCK), 1))
                gap = jnp.abs(q_place - k_place)
                mid = (gap % mid_step == 0) & (gap <= SIDE_SPAN * mid_step)
                wide = (gap % wide_step == 0) & (gap <= SIDE_SPAN * wide_step)
                bias_class[
                    a * ROW_BLOCK : (a + 1) * ROW_BLOCK, b * ROW_BLOCK : (b + 1) * ROW_BLOCK
                ] = jnp.where(
                    mid & wide, float(np.log(2.0)), jnp.where(mid | wide, 0.0, NEGATIVE)
                )

    def turn(x, cos, sin):
        swapped = jnp.where(
            front, pltpu.roll(x, PAIR - HEAD_DIM // 2, 1), pltpu.roll(x, HEAD_DIM // 2, 1)
        )
        return x * cos + swapped * sin

    def project(seg, n):
        if len(spans[seg]) == 1:
            left = x_all[spans[seg][0][0]]
        else:
            left = jnp.concatenate([x_all[s, pl.ds(a, c)] for s, a, c in spans[seg]], axis=0)
        full = jnp.dot(left, w_all[n], preferred_element_type=f32)
        at = 0
        for s, a, c in spans[seg]:
            r0 = row_of(s, a, c)
            if n != V:
                cos = cos_t[pl.ds(r0, c)]
                sin = sin_t[pl.ds(r0, c)]
            for g in range(group_count):
                part = full[at : at + c, g * PAIR : (g + 1) * PAIR]
                if n != V:
                    part = turn(part, cos, sin)
                pf[n * group_count + g, seg * shard + at : seg * shard + at + c, :] = part
                low = part.astype(bf16)
                if n == Q:
                    q_c[pl.ds(r0, c), g * PAIR : (g + 1) * PAIR] = low
                else:
                    kv_ext[
                        pl.ds(r0 + SIDE_SPAN, c),
                        n * col_count + g * PAIR : n * col_count + (g + 1) * PAIR,
                    ] = low
            at += c

    a2a = {}

    def scatter(unit):
        seg, names = UNITS[unit]
        span = slice(seg * share, (seg + 1) * share)
        cols = slice(names[0] * col_count, (names[-1] + 1) * col_count)

        def one(r, carry):
            for g in range(names[0] * group_count, (names[-1] + 1) * group_count):
                cls_send[r, span, g * PAIR : (g + 1) * PAIR] = pf[
                    g, pl.ds(seg * shard + r, share, stride=sp_size), :
                ].astype(bf16)
            return carry

        lax.fori_loop(0, sp_size, one, 0)
        mine = pl.ds(pl.multiple_of(seg * shard + sp * share, share), share)
        for off in offsets:
            dest = (sp + off) % sp_size
            a2a[unit, off] = launch(
                remote(
                    cls_send.at[dest, span, cols], cls_recv.at[mine, cols],
                    a2a_send.at[unit, off], a2a_recv.at[unit, off], sp=dest,
                )
            )
        cls_recv[mine, cols] = cls_send[sp, span, cols]

    def gathered(*units):
        for unit in units:
            for off in offsets:
                a2a[unit, off].wait_recv()

    def edge(which, n):
        src = pl.multiple_of(SIDE_SPAN + which * (rows - SIDE_SPAN), SIDE_SPAN)
        dst = pl.multiple_of((1 - which) * (rows + SIDE_SPAN), SIDE_SPAN)
        return launch(
            remote(
                kv_ext.at[pl.ds(src, SIDE_SPAN)], kv_ext.at[pl.ds(dst, SIDE_SPAN)],
                halo_send.at[n], halo_recv.at[n], sp=(sp + sp_size - 1 + 2 * which) % sp_size,
            )
        )

    load_x.wait()
    load_w[K].wait()
    project(0, K)
    load_w[V].wait()
    project(0, V)
    scatter(0)
    own.wait_recv()
    project(1, K)
    project(1, V)
    scatter(1)
    halo_early = edge(chip, 0)
    load_w[Q].wait()
    project(0, Q)
    project(1, Q)

    fwd = []
    for k in range(SPLITS):
        span = pl.ds(k * piece, piece)
        far[k].wait_recv()
        fwd.append(
            launch(
                remote(
                    x_all.at[far_same, span], x_all.at[far_same, span],
                    fwd_send.at[k], fwd_recv.at[k], tp=partner,
                )
            )
        )
        if k == 0:
            build_bias()
        fwd[k].wait_recv()
        project(2 + k, K)
        project(2 + k, V)
        if k == 0:
            project(2, Q)
            scatter(2)
            scatter(3)
        else:
            scatter(4)
            project(3, Q)
            scatter(5)
    halo_late = edge(1 - chip, 1)

    lane_wide = lax.broadcasted_iota(jnp.int32, (ROW_BLOCK, PAIR), 1)
    scale = HEAD_DIM ** (-0.5)

    def attend(query, keys, values, bias):
        outs, sums = [], []
        for half in range(2):
            pick = first_head if half == 0 else jnp.logical_not(first_head)
            q = jnp.where(pick, query.astype(f32) * scale, 0.0).astype(bf16)
            s = lax.dot_general(q, keys, (((1,), (1,)), ((), ())), preferred_element_type=f32)
            s = s + bias
            top = jnp.max(s, axis=1, keepdims=True)
            e = jnp.exp(s - top)
            total = jnp.sum(e, axis=1, keepdims=True)
            o = jnp.dot(e.astype(bf16), values, preferred_element_type=f32)
            outs.append(o / total)
            sums.append(top + jnp.log(total))
        return jnp.where(first_head, outs[0], outs[1]), sums

    def keep_sums(ref, span, g, sums):
        kept = ref[span]
        kept = jnp.where(lane_wide == 2 * g, sums[0], kept)
        ref[span] = jnp.where(lane_wide == 2 * g + 1, sums[1], kept)

    def near(shards):
        def pair(g, carry):
            c0 = pl.multiple_of(g * PAIR, PAIR)
            for s in shards:
                r0 = row_of(s, 0, shard)
                span = pl.ds(r0, ROW_BLOCK)
                o, sums = attend(
                    q_c[span, pl.ds(c0, PAIR)],
                    kv_ext[pl.ds(r0, window), pl.ds(c0, PAIR)],
                    kv_ext[pl.ds(r0, window), pl.ds(c0 + col_count, PAIR)],
                    bias_near[span],
                )
                o_near[g, span, :] = o
                keep_sums(lse_near, span, g, sums)
            return carry

        lax.fori_loop(0, group_count, pair, 0)

    my_share = pl.ds(pl.multiple_of(sp * share, share), share)
    back, lback = {}, {}

    def class_attend(seg):
        span = slice(seg * shard, (seg + 1) * shard)

        def block(g):
            c0 = pl.multiple_of(g * PAIR, PAIR)
            o, sums = attend(
                cls_recv[span, pl.ds(c0 + Q * col_count, PAIR)],
                cls_recv[:, pl.ds(c0 + K * col_count, PAIR)],
                cls_recv[:, pl.ds(c0 + V * col_count, PAIR)],
                bias_class[span],
            )
            cls_o[span, pl.ds(c0, PAIR)] = o.astype(bf16)
            keep_sums(cls_lse, span, g, sums)

        def two(i, carry):
            block(2 * i)
            block(2 * i + 1)
            return carry

        lax.fori_loop(0, group_count // 2, two, 0)
        lse_out[seg] = jnp.transpose(cls_lse[span])[:head_count]
        for off in offsets:
            dest = (sp + off) % sp_size
            part = pl.ds(pl.multiple_of(seg * shard + dest * share, share), share)
            back[seg, off] = launch(
                remote(
                    cls_o.at[part], ret.at[seg, my_share],
                    back_send.at[seg, off], back_recv.at[seg, off], sp=dest,
                )
            )
            lback[seg, off] = launch(
                remote(
                    lse_out.at[seg], ret_lse.at[seg, sp],
                    lback_send.at[seg, off], lback_recv.at[seg, off], sp=dest,
                )
            )
        mine = pl.ds(pl.multiple_of(seg * shard + sp * share, share), share)
        ret[seg, my_share] = cls_o[mine]
        ret_lse[seg, sp] = lse_out[seg]

    head_lane = lax.broadcasted_iota(jnp.int32, (head_count, PAIR), 1)

    def gather_rows(ref, seg):
        return jnp.concatenate([ref[pl.ds(row_of(s, a, c), c)] for s, a, c in spans[seg]], axis=0)

    def combine(seg):
        for off in offsets:
            lback[seg, off].wait_recv()
        flat = jnp.zeros((head_count, PAIR), f32)
        for r in range(sp_size):
            moved = pltpu.roll(ret_lse[seg, r], (r - sp + sp_size) % sp_size * share, 1)
            flat = jnp.where(head_lane // share == r, moved, flat)
        tall = jnp.transpose(
            jnp.concatenate([flat, jnp.zeros((PAIR - head_count, PAIR), f32)], axis=0)
        )
        for r in range(sp_size):
            lse_f[pl.ds(r, share, stride=sp_size), :] = tall[r * share : (r + 1) * share]
        for off in offsets:
            back[seg, off].wait_recv()
        for g in range(group_count):
            for r in range(sp_size):
                ret_f[g, pl.ds(r, share, stride=sp_size), :] = ret[
                    seg, r * share : (r + 1) * share, g * PAIR : (g + 1) * PAIR
                ].astype(f32)
        la = gather_rows(lse_near, seg)
        lb = lse_f[...]
        peak = jnp.maximum(la, lb)
        ea = jnp.exp(la - peak)
        eb = jnp.exp(lb - peak)
        total = ea + eb
        logw = jnp.transpose(peak + jnp.log(total))[:head_count]
        if seg < 2:
            logw_ref[:, pl.ds(row_of(*spans[seg][0]), shard)] = logw
        else:
            logw_far[seg - 2] = logw
        ea = ea / total
        eb = eb / total
        for g in range(group_count):
            wa = jnp.where(first_head, ea[:, 2 * g : 2 * g + 1], ea[:, 2 * g + 1 : 2 * g + 2])
            wb = jnp.where(first_head, eb[:, 2 * g : 2 * g + 1], eb[:, 2 * g + 1 : 2 * g + 2])
            mixed = wa * gather_rows(o_near.at[g], seg) + wb * ret_f[g]
            att[seg, :, g * PAIR : (g + 1) * PAIR] = mixed.astype(bf16)

    width = wo.shape[1] // OUT_SPLITS

    def product(seg, n):
        return jnp.dot(
            att[seg], wo[:, n * width : (n + 1) * width], preferred_element_type=f32
        ).astype(bf16)

    exch, cross, own_exch = {}, {}, {}

    def relay(k, n):
        exch[k, n].wait_recv()
        cross_out[k, n] = (keep_b[k, n].astype(f32) + part_in[k, n].astype(f32)).astype(bf16)
        cross[k, n] = launch(
            remote(
                cross_out.at[k, n], cross_in.at[k, n], cr_send.at[k, n], cr_recv.at[k, n],
                tp=far_same,
            )
        )

    def out_far(k):
        for n in range(OUT_SPLITS):
            both = product(2 + k, n)
            part_out[k, n] = both[piece:]
            exch[k, n] = launch(
                remote(
                    part_out.at[k, n], part_in.at[k, n], ex_send.at[k, n], ex_recv.at[k, n],
                    tp=partner,
                )
            )
            keep_b[k, n] = both[:piece]
            if n:
                relay(k, n - 1)
        relay(k, OUT_SPLITS - 1)

    lse_near[...] = jnp.zeros_like(lse_near)
    cls_lse[...] = jnp.zeros_like(cls_lse)
    halo_early.wait_recv()
    near((far_same, far_other))
    gathered(0, 1, 2, 4)
    class_attend(2)
    scatter(6)
    gathered(5)
    class_attend(3)
    load_out.wait()
    combine(2)
    out_far(0)
    combine(3)
    out_far(1)
    first_half = head_lane < piece
    swap = [pltpu.roll(logw_far[k], piece, 1) for k in range(SPLITS)]
    logw_ref[:, pl.ds(row_of(far_same, 0, shard), shard)] = jnp.where(
        first_half, logw_far[0], swap[1]
    )
    logw_ref[:, pl.ds(row_of(far_other, 0, shard), shard)] = jnp.where(
        first_half, swap[0], logw_far[1]
    )
    gathered(3)
    class_attend(0)
    gathered(6)
    class_attend(1)
    halo_late.wait_recv()
    near((tp, partner))
    combine(1)
    for n in range(OUT_SPLITS):
        own_out[n] = product(1, n)
        own_exch[n] = launch(
            remote(own_out.at[n], own_in.at[n], ox_send.at[n], ox_recv.at[n], tp=partner)
        )
    combine(0)
    for n in range(OUT_SPLITS):
        keep_d[n] = product(0, n).astype(f32)
    for n in range(OUT_SPLITS):
        own_exch[n].wait_recv()
        keep_d[n] = keep_d[n] + own_in[n].astype(f32)
    for k in range(SPLITS):
        for n in range(OUT_SPLITS):
            cross[k, n].wait_recv()
            out_ref[k * piece : (k + 1) * piece, n * width : (n + 1) * width] = (
                keep_d[n, k * piece : (k + 1) * piece] + cross_in[k, n].astype(f32)
            ).astype(bf16)

    for item in waits:
        item.wait_send()


def fused(sp_size, tp_size, tokens_in, w_query, w_key, w_value, w_out):
    shard, depth = tokens_in.shape
    col_count = w_query.shape[1]
    rows = shard * tp_size
    groups = col_count // PAIR
    heads = col_count // HEAD_DIM
    share = shard // sp_size
    piece = shard // SPLITS
    wide = w_out.shape[1]
    width = wide // OUT_SPLITS
    half = HEAD_DIM // 2
    freq = 1.0 / ROTARY_BASE ** (np.arange(half) / half)
    freq = np.tile(freq, PAIR // half)
    start = np.concatenate([np.arange(rows), np.arange(sp_size) * rows])
    angle = start[:, None] * freq[None, :]
    table = jnp.asarray(np.stack([np.cos(angle), np.sin(angle)]).astype(np.float32))
    f32, bf16 = jnp.float32, jnp.bfloat16
    V_, DMA = pltpu.VMEM, pltpu.SemaphoreType.DMA
    window = ROW_BLOCK + 2 * SIDE_SPAN
    scratch = [
        V_((tp_size, shard, depth), bf16),
        V_((3, depth, col_count), bf16),
        V_((col_count, wide), bf16),
        V_(table.shape, f32),
        V_((rows, PAIR), f32),
        V_((rows, PAIR), f32),
        V_((rows, col_count), bf16),
        V_((rows + 2 * SIDE_SPAN, 2 * col_count), bf16),
        V_((3 * groups, rows, PAIR), f32),
        V_((sp_size, SEGMENTS * share, 3 * col_count), bf16),
        V_((rows, 3 * col_count), bf16),
        V_((rows, window), f32),
        V_((rows, rows), f32),
        V_((groups, rows, PAIR), f32),
        V_((rows, PAIR), f32),
        V_((rows, col_count), bf16),
        V_((rows, PAIR), f32),
        V_((SEGMENTS, heads, PAIR), f32),
        V_((SEGMENTS, shard, col_count), bf16),
        V_((SEGMENTS, sp_size, heads, PAIR), f32),
        V_((groups, shard, PAIR), f32),
        V_((shard, PAIR), f32),
        V_((SPLITS, heads, PAIR), f32),
        V_((SEGMENTS, shard, col_count), bf16),
        V_((SPLITS, OUT_SPLITS, piece, width), bf16),
        V_((SPLITS, OUT_SPLITS, piece, width), bf16),
        V_((SPLITS, OUT_SPLITS, piece, width), bf16),
        V_((SPLITS, OUT_SPLITS, piece, width), bf16),
        V_((SPLITS, OUT_SPLITS, piece, width), bf16),
        V_((OUT_SPLITS, shard, width), f32),
        V_((OUT_SPLITS, shard, width), bf16),
        V_((OUT_SPLITS, shard, width), bf16),
        DMA((6,)),
        DMA((1,)), DMA((1,)),
        DMA((SPLITS,)), DMA((SPLITS,)),
        DMA((SPLITS,)), DMA((SPLITS,)),
        DMA((len(UNITS), sp_size)), DMA((len(UNITS), sp_size)),
        DMA((2,)), DMA((2,)),
        DMA((SEGMENTS, sp_size)), DMA((SEGMENTS, sp_size)),
        DMA((SEGMENTS, sp_size)), DMA((SEGMENTS, sp_size)),
        DMA((SPLITS, OUT_SPLITS)), DMA((SPLITS, OUT_SPLITS)),
        DMA((SPLITS, OUT_SPLITS)), DMA((SPLITS, OUT_SPLITS)),
        DMA((OUT_SPLITS,)), DMA((OUT_SPLITS,)),
    ]
    hbm = pl.BlockSpec(memory_space=pltpu.HBM)
    vmem = pl.BlockSpec(memory_space=pltpu.VMEM)
    return pl.pallas_call(
        functools.partial(class_kernel, sp_size, tp_size, col_count),
        out_shape=(
            jax.ShapeDtypeStruct((shard, wide), bf16),
            jax.ShapeDtypeStruct((heads, rows), f32),
        ),
        in_specs=[hbm] * 6,
        out_specs=(vmem, vmem),
        scratch_shapes=scratch,
        compiler_params=pltpu.CompilerParams(
            collective_id=0, has_side_effects=True, vmem_limit_bytes=VMEM_GRANT
        ),
        name="dilated_layer",
    )(tokens_in, w_query, w_key, w_value, w_out, table)


VMEM_GRANT = 52 * 1024 * 1024


def solution(mesh):
    in_specs = (P(("sp", "tp"), None), P(None, "tp"), P(None, "tp"), P(None, "tp"), P("tp", None))
    out_specs = (P(("sp", "tp"), None), P("tp", "sp"))
    sp_size, tp_size = mesh.shape["sp"], mesh.shape["tp"]

    def body(*args):
        shard = args[0].shape[0]
        whole_class = (
            MIDDLE_DILATION % sp_size == 0
            and WIDEST_DILATION % sp_size == 0
            and tp_size == 2 * SPLITS
            and shard == ROW_BLOCK
            and shard % (16 * sp_size) == 0
            and args[1].shape[1] % (2 * PAIR) == 0
        )
        if whole_class:
            return fused(sp_size, tp_size, *args)
        return per_device(*args)

    return jax.shard_map(body, mesh=mesh, in_specs=in_specs, out_specs=out_specs, check_vma=False)
```

```python
import functools

import jax
import jax.numpy as jnp
import numpy as np
from jax import lax
from jax.experimental import pallas as pl
from jax.experimental.pallas import tpu as pltpu
from jax.sharding import PartitionSpec as P

HEAD_DIM = 64
SIDE_SPAN = 64
MIDDLE_DILATION = 8
WIDEST_DILATION = 64


ROTARY_BASE = 500000.0
NEGATIVE = -1e30


def shifted(block, axis, distance):
    devices = range(lax.axis_size(axis))
    route = [(i - distance, i) for i in devices if i - distance in devices]
    return lax.ppermute(block, axis, route)


def rotate(block, positions):
    half_size = block.shape[-1] // 2
    freq = 1.0 / ROTARY_BASE ** (jnp.arange(half_size, dtype=jnp.float32) / half_size)
    angle = positions[:, None] * freq[None, :]
    cosine = jnp.cos(angle)[:, None, :]
    sine = jnp.sin(angle)[:, None, :]
    front = block[..., :half_size]
    back = block[..., half_size:]
    return jnp.concatenate([front * cosine - back * sine, back * cosine + front * sine], axis=-1)


def pattern_attend(query, keys, values, lead_rows, dilation_step, low_row, high_row):
    rows_total, head_count, head_size = query.shape
    class_len = rows_total // dilation_step
    first_class = lead_rows // dilation_step - SIDE_SPAN
    class_q = query.reshape(class_len, dilation_step, head_count, head_size)
    class_k = keys.reshape(keys.shape[0] // dilation_step, dilation_step, head_count, head_size)
    class_v = values.reshape(values.shape[0] // dilation_step, dilation_step, head_count, head_size)
    sub_k = class_k[first_class : first_class + class_len + 2 * SIDE_SPAN]
    sub_v = class_v[first_class : first_class + class_len + 2 * SIDE_SPAN]
    if class_len <= SIDE_SPAN:
        block_len = class_len
        block_count = 1
        win_k = sub_k[None]
        win_v = sub_v[None]
        blocks_q = class_q[None]
    else:
        block_len = SIDE_SPAN
        block_count = class_len // SIDE_SPAN
        part_k = sub_k.reshape(block_count + 2, SIDE_SPAN, dilation_step, head_count, head_size)
        part_v = sub_v.reshape(block_count + 2, SIDE_SPAN, dilation_step, head_count, head_size)
        win_k = jnp.concatenate([part_k[:-2], part_k[1:-1], part_k[2:]], axis=1)
        win_v = jnp.concatenate([part_v[:-2], part_v[1:-1], part_v[2:]], axis=1)
        blocks_q = class_q.reshape(block_count, SIDE_SPAN, dilation_step, head_count, head_size)
    width = block_len + 2 * SIDE_SPAN
    scores = jnp.einsum("nasht,nksht->nshak", blocks_q, win_k, preferred_element_type=jnp.float32)
    scores = scores * head_size ** (-0.5)
    q_index = jnp.arange(block_len, dtype=jnp.int32)
    k_index = jnp.arange(width, dtype=jnp.int32)
    b_index = jnp.arange(block_count, dtype=jnp.int32)
    s_index = jnp.arange(dilation_step, dtype=jnp.int32)
    in_band = jnp.abs(k_index[None, :] - SIDE_SPAN - q_index[:, None]) <= SIDE_SPAN
    key_position = (
        (first_class + b_index[:, None] * block_len + k_index[None, :]) * dilation_step
    )[:, None, :] + s_index[None, :, None]
    is_valid = (key_position >= low_row) & (key_position < high_row)
    keep_mask = in_band[None, None, None] & is_valid[:, :, None, None, :]
    scores = jnp.where(keep_mask, scores, NEGATIVE)
    maxima = jnp.max(scores, axis=-1, keepdims=True)
    expo = jnp.exp(scores - maxima)
    totals = jnp.sum(expo, axis=-1)
    numerator = jnp.einsum(
        "nshak,nksht->nasht", expo.astype(jnp.bfloat16), win_v, preferred_element_type=jnp.float32
    )
    totals_t = jnp.transpose(totals, (0, 3, 1, 2))
    result = (
        (numerator / totals_t[..., None])
        .astype(jnp.bfloat16)
        .reshape(rows_total, head_count, head_size)
    )
    log_sum = jnp.transpose(maxima[..., 0] + jnp.log(totals), (0, 3, 1, 2)).reshape(
        rows_total, head_count
    )
    return (result, log_sum)


def combine(results):
    sums = jnp.stack([item[1] for item in results], axis=0)
    peak = jnp.max(sums, axis=0)
    share = jnp.exp(sums - peak[None])
    weight_sum = share[0] + share[1] + share[2]
    accum = share[0][..., None] * results[0][0].astype(jnp.float32)
    accum = accum + share[1][..., None] * results[1][0].astype(jnp.float32)
    accum = accum + share[2][..., None] * results[2][0].astype(jnp.float32)
    attended = (accum / weight_sum[..., None]).astype(jnp.bfloat16)
    return (attended, peak + jnp.log(weight_sum))


def per_device(tokens_in, w_query, w_key, w_value, w_out):
    col_count = w_query.shape[1]
    head_count = col_count // HEAD_DIM
    piece = lax.all_gather(tokens_in, "tp", axis=0, tiled=True)
    projected = jnp.concatenate(
        [
            jnp.dot(piece, w_query, preferred_element_type=jnp.float32),
            jnp.dot(piece, w_key, preferred_element_type=jnp.float32),
            jnp.dot(piece, w_value, preferred_element_type=jnp.float32),
        ],
        axis=1,
    )
    rows_total = projected.shape[0]
    sp_size = lax.axis_size("sp")
    sp_place = lax.axis_index("sp")
    positions = (sp_place * rows_total + jnp.arange(rows_total, dtype=jnp.int32)).astype(
        jnp.float32
    )
    shape3 = (rows_total, head_count, HEAD_DIM)
    query = rotate(projected[:, :col_count].reshape(shape3), positions).astype(jnp.bfloat16)
    keys = rotate(projected[:, col_count : 2 * col_count].reshape(shape3), positions).astype(
        jnp.bfloat16
    )
    values = projected[:, 2 * col_count :].astype(jnp.bfloat16).reshape(shape3)
    per_device_span = -(-(SIDE_SPAN * MIDDLE_DILATION) // rows_total)
    earlier_k = []
    earlier_v = []
    before_k, before_v = shifted((keys, values), "sp", 1)
    after_k, after_v = shifted((keys, values), "sp", -1)
    earlier_k.insert(0, before_k)
    earlier_v.insert(0, before_v)
    later_k = [after_k]
    later_v = [after_v]
    key_buf = jnp.concatenate(earlier_k + [keys] + later_k, axis=0)
    value_buf = jnp.concatenate(earlier_v + [values] + later_v, axis=0)
    lead_rows = per_device_span * rows_total
    low_row = lead_rows - sp_place * rows_total
    key_buf, value_buf, lead_rows, low_row, high_row = (
        key_buf,
        value_buf,
        lead_rows,
        low_row,
        low_row + sp_size * rows_total,
    )
    results = [
        pattern_attend(query, key_buf, value_buf, lead_rows, dilation_step, low_row, high_row)
        for dilation_step in (1, MIDDLE_DILATION)
    ]
    class_stride = WIDEST_DILATION // sp_size
    border_extent = SIDE_SPAN * class_stride
    class_shape = (rows_total // sp_size, sp_size, head_count, HEAD_DIM)
    parts = (
        lax.all_to_all(query.reshape(class_shape), "sp", split_axis=1, concat_axis=0, tiled=True),
        lax.all_to_all(keys.reshape(class_shape), "sp", split_axis=1, concat_axis=0, tiled=True),
        lax.all_to_all(values.reshape(class_shape), "sp", split_axis=1, concat_axis=0, tiled=True),
    )
    item_heads = parts[0].shape[2]
    flat = [item.reshape(rows_total, item_heads, HEAD_DIM) for item in parts]
    pad_k = jnp.pad(flat[1], ((border_extent, border_extent), (0, 0), (0, 0)))
    pad_v = jnp.pad(flat[2], ((border_extent, border_extent), (0, 0), (0, 0)))
    result, log_sum = pattern_attend(
        flat[0],
        pad_k,
        pad_v,
        border_extent,
        class_stride,
        border_extent,
        border_extent + rows_total,
    )
    result_back = lax.all_to_all(
        result.reshape(rows_total, 1, item_heads, HEAD_DIM),
        "sp",
        split_axis=0,
        concat_axis=1,
        tiled=True,
    )
    sum_back = lax.all_to_all(
        log_sum.reshape(rows_total, 1, item_heads), "sp", split_axis=0, concat_axis=1, tiled=True
    )
    results.append((result_back.reshape(shape3), sum_back.reshape(rows_total, head_count)))
    attended, log_weight = combine(results)
    flat_out = attended.reshape(rows_total, col_count)
    mixed = lax.psum_scatter(
        jnp.dot(flat_out, w_out, preferred_element_type=jnp.float32).astype(jnp.bfloat16),
        "tp",
        scatter_dimension=0,
        tiled=True,
    )
    return (mixed, jnp.transpose(log_weight, (1, 0)))


MESH_ID = pl.DeviceIdType.MESH
PAIR = 2 * HEAD_DIM
ROW_BLOCK = 128
SPLITS = 2
OUT_SPLITS = 4
SEGMENTS = 4
K, V, Q = 0, 1, 2
UNITS = ((0, (K, V)), (1, (K, V)), (0, (Q,)), (1, (Q,)), (2, (K, V, Q)), (3, (K, V)), (3, (Q,)))


def class_kernel(
    sp_size, tp_size, col_count,
    x_hbm, wq_hbm, wk_hbm, wv_hbm, wo_hbm, table_hbm,
    out_ref, logw_ref,
    x_all, w_all, wo, table, cos_t, sin_t, q_c, kv_ext, pf, cls_send, cls_recv,
    bias_near, bias_class, o_near, lse_near, cls_o, cls_lse, lse_out, ret, ret_lse, ret_f, lse_f, logw_far,
    att, part_out, part_in, cross_out, cross_in, keep_b, keep_d, own_out, own_in,
    load_sem, own_send, own_recv, far_send, far_recv, fwd_send, fwd_recv,
    a2a_send, a2a_recv, halo_send, halo_recv, back_send, back_recv, lback_send, lback_recv,
    ex_send, ex_recv, cr_send, cr_recv, ox_send, ox_recv,
):
    sp = lax.axis_index("sp")
    tp = lax.axis_index("tp")
    chip = tp // 2
    core = tp % 2
    partner = chip * 2 + (1 - core)
    far_same = (1 - chip) * 2 + core
    far_other = (1 - chip) * 2 + (1 - core)
    shard = x_hbm.shape[0]
    rows = shard * tp_size
    piece = shard // SPLITS
    group_count = col_count // PAIR
    head_count = col_count // HEAD_DIM
    share = shard // sp_size
    f32, bf16 = jnp.float32, jnp.bfloat16

    offsets = sorted(range(1, sp_size), key=lambda off: (abs(off - sp_size // 2), off))

    spans = (
        ((tp, 0, shard),),
        ((partner, 0, shard),),
        ((far_same, 0, piece), (far_other, 0, piece)),
        ((far_same, piece, piece), (far_other, piece, piece)),
    )

    def row_of(s, a, c):
        return pl.multiple_of(s * shard + a, c)

    load_table = pltpu.make_async_copy(table_hbm.at[0:2], table, load_sem.at[0])
    load_x = pltpu.make_async_copy(x_hbm, x_all.at[tp], load_sem.at[1])
    load_w = [
        pltpu.make_async_copy(w, w_all.at[n], load_sem.at[2 + n])
        for n, w in enumerate((wk_hbm, wv_hbm, wq_hbm))
    ]
    load_out = pltpu.make_async_copy(wo_hbm, wo, load_sem.at[5])
    load_x.start()
    load_table.start()
    for item in load_w:
        item.start()

    barrier = pltpu.get_barrier_semaphore()
    pl.semaphore_signal(barrier, inc=1, device_id={"tp": partner}, device_id_type=MESH_ID)
    pl.semaphore_signal(barrier, inc=1, device_id={"tp": far_same}, device_id_type=MESH_ID)
    for off in offsets:
        pl.semaphore_signal(
            barrier, inc=1, device_id={"sp": (sp + off) % sp_size}, device_id_type=MESH_ID
        )
    pl.semaphore_wait(barrier, 2 + (sp_size - 1))

    def remote(src, dst, send, recv, **where):
        return pltpu.make_async_remote_copy(
            src_ref=src, dst_ref=dst, send_sem=send, recv_sem=recv,
            device_id=where, device_id_type=MESH_ID,
        )

    waits = []

    def launch(item):
        item.start()
        waits.append(item)
        return item

    far = []
    for k in range(SPLITS):
        span = pl.ds(k * piece, piece)
        far.append(
            launch(
                remote(
                    x_hbm.at[span], x_all.at[tp, span], far_send.at[k], far_recv.at[k], tp=far_same
                )
            )
        )
    own = launch(remote(x_hbm, x_all.at[tp], own_send.at[0], own_recv.at[0], tp=partner))
    load_out.start()

    lane = lax.broadcasted_iota(jnp.int32, (1, PAIR), 1)
    front = lane % HEAD_DIM < HEAD_DIM // 2
    first_head = lane < HEAD_DIM
    sign = jnp.where(front, -1.0, 1.0).astype(f32)
    load_table.wait()
    base_cos = table[0, pl.ds(rows + sp, 1), :]
    base_sin = table[1, pl.ds(rows + sp, 1), :]
    for r0 in range(0, rows, ROW_BLOCK):
        lc = table[0, r0 : r0 + ROW_BLOCK]
        ls = table[1, r0 : r0 + ROW_BLOCK]
        cos_t[r0 : r0 + ROW_BLOCK] = lc * base_cos - ls * base_sin
        sin_t[r0 : r0 + ROW_BLOCK] = (ls * base_cos + lc * base_sin) * sign

    window = ROW_BLOCK + 2 * SIDE_SPAN
    mid_step = MIDDLE_DILATION // sp_size
    wide_step = WIDEST_DILATION // sp_size
    per_source = rows // sp_size
    half_share = share // 2

    def place_of(seg, index):
        source = index // share
        j = index % share
        if seg < 2:
            inner = spans[seg][0][0] * share + j
        else:
            inner = jnp.where(
                j < half_share,
                far_same * share + (seg - 2) * half_share + j,
                far_other * share + (seg - 3) * half_share + j,
            )
        return source * per_source + inner

    def build_bias():
        near_i = lax.broadcasted_iota(jnp.int32, (ROW_BLOCK, window), 0)
        near_j = lax.broadcasted_iota(jnp.int32, (ROW_BLOCK, window), 1)
        near_band = jnp.abs(near_j - SIDE_SPAN - near_i) <= SIDE_SPAN
        for r0 in range(0, rows, ROW_BLOCK):
            key_pos = sp * rows + r0 + near_j - SIDE_SPAN
            good = near_band & (key_pos >= 0) & (key_pos < sp_size * rows)
            bias_near[r0 : r0 + ROW_BLOCK] = jnp.where(good, 0.0, NEGATIVE)
        for a in range(SEGMENTS):
            q_place = place_of(a, lax.broadcasted_iota(jnp.int32, (ROW_BLOCK, 1), 0))
            for b in range(SEGMENTS):
                k_place = place_of(b, lax.broadcasted_iota(jnp.int32, (1, ROW_BLOCK), 1))
                gap = jnp.abs(q_place - k_place)
                mid = (gap % mid_step == 0) & (gap <= SIDE_SPAN * mid_step)
                wide = (gap % wide_step == 0) & (gap <= SIDE_SPAN * wide_step)
                bias_class[
                    a * ROW_BLOCK : (a + 1) * ROW_BLOCK, b * ROW_BLOCK : (b + 1) * ROW_BLOCK
                ] = jnp.where(
                    mid & wide, float(np.log(2.0)), jnp.where(mid | wide, 0.0, NEGATIVE)
                )

    def turn(x, cos, sin):
        swapped = jnp.where(
            front, pltpu.roll(x, PAIR - HEAD_DIM // 2, 1), pltpu.roll(x, HEAD_DIM // 2, 1)
        )
        return x * cos + swapped * sin

    def project(seg, n):
        if len(spans[seg]) == 1:
            left = x_all[spans[seg][0][0]]
        else:
            left = jnp.concatenate([x_all[s, pl.ds(a, c)] for s, a, c in spans[seg]], axis=0)
        full = jnp.dot(left, w_all[n], preferred_element_type=f32)
        at = 0
        for s, a, c in spans[seg]:
            r0 = row_of(s, a, c)
            if n != V:
                cos = cos_t[pl.ds(r0, c)]
                sin = sin_t[pl.ds(r0, c)]
            for g in range(group_count):
                part = full[at : at + c, g * PAIR : (g + 1) * PAIR]
                if n != V:
                    part = turn(part, cos, sin)
                pf[n * group_count + g, seg * shard + at : seg * shard + at + c, :] = part
                low = part.astype(bf16)
                if n == Q:
                    q_c[pl.ds(r0, c), g * PAIR : (g + 1) * PAIR] = low
                else:
                    kv_ext[
                        pl.ds(r0 + SIDE_SPAN, c),
                        n * col_count + g * PAIR : n * col_count + (g + 1) * PAIR,
                    ] = low
            at += c

    def bulk(ref, send, recv):
        return remote(ref, ref, send, recv, tp=partner)

    others = (sp_size - 1) * share

    def a2a_total(unit):
        seg, names = UNITS[unit]
        cols = slice(names[0] * col_count, (names[-1] + 1) * col_count)
        return bulk(
            cls_recv.at[pl.ds(seg * shard, others), cols], a2a_send.at[unit], a2a_recv.at[unit]
        )

    def scatter(unit):
        seg, names = UNITS[unit]
        span = slice(seg * share, (seg + 1) * share)
        cols = slice(names[0] * col_count, (names[-1] + 1) * col_count)

        def one(r, carry):
            for g in range(names[0] * group_count, (names[-1] + 1) * group_count):
                cls_send[r, span, g * PAIR : (g + 1) * PAIR] = pf[
                    g, pl.ds(seg * shard + r, share, stride=sp_size), :
                ].astype(bf16)
            return carry

        lax.fori_loop(0, sp_size, one, 0)
        mine = pl.ds(pl.multiple_of(seg * shard + sp * share, share), share)
        for off in offsets:
            dest = (sp + off) % sp_size
            remote(
                cls_send.at[dest, span, cols], cls_recv.at[mine, cols],
                a2a_send.at[unit], a2a_recv.at[unit], sp=dest,
            ).start()
        waits.append(a2a_total(unit))
        cls_recv[mine, cols] = cls_send[sp, span, cols]

    def gathered(*units):
        for unit in units:
            a2a_total(unit).wait_recv()

    def edge(which, n):
        src = pl.multiple_of(SIDE_SPAN + which * (rows - SIDE_SPAN), SIDE_SPAN)
        dst = pl.multiple_of((1 - which) * (rows + SIDE_SPAN), SIDE_SPAN)
        return launch(
            remote(
                kv_ext.at[pl.ds(src, SIDE_SPAN)], kv_ext.at[pl.ds(dst, SIDE_SPAN)],
                halo_send.at[n], halo_recv.at[n], sp=(sp + sp_size - 1 + 2 * which) % sp_size,
            )
        )

    load_x.wait()
    load_w[K].wait()
    project(0, K)
    load_w[V].wait()
    project(0, V)
    scatter(0)
    own.wait_recv()
    project(1, K)
    project(1, V)
    scatter(1)
    halo_early = edge(chip, 0)
    load_w[Q].wait()
    project(0, Q)
    scatter(2)
    project(1, Q)
    scatter(3)

    fwd = []
    for k in range(SPLITS):
        span = pl.ds(k * piece, piece)
        far[k].wait_recv()
        fwd.append(
            launch(
                remote(
                    x_all.at[far_same, span], x_all.at[far_same, span],
                    fwd_send.at[k], fwd_recv.at[k], tp=partner,
                )
            )
        )
        if k == 0:
            build_bias()
        fwd[k].wait_recv()
        project(2 + k, K)
        project(2 + k, V)
        if k == 0:
            project(2, Q)
            scatter(4)
        else:
            scatter(5)
            project(3, Q)

    lane_wide = lax.broadcasted_iota(jnp.int32, (ROW_BLOCK, PAIR), 1)
    scale = HEAD_DIM ** (-0.5)

    def attend(query, keys, values, bias):
        outs, sums = [], []
        for half in range(2):
            pick = first_head if half == 0 else jnp.logical_not(first_head)
            q = jnp.where(pick, query.astype(f32) * scale, 0.0).astype(bf16)
            s = lax.dot_general(q, keys, (((1,), (1,)), ((), ())), preferred_element_type=f32)
            s = s + bias
            top = jnp.max(s, axis=1, keepdims=True)
            e = jnp.exp(s - top)
            total = jnp.sum(e, axis=1, keepdims=True)
            o = jnp.dot(e.astype(bf16), values, preferred_element_type=f32)
            outs.append(o / total)
            sums.append(top + jnp.log(total))
        return jnp.where(first_head, outs[0], outs[1]), sums

    def keep_sums(ref, span, g, sums):
        kept = ref[span]
        kept = jnp.where(lane_wide == 2 * g, sums[0], kept)
        ref[span] = jnp.where(lane_wide == 2 * g + 1, sums[1], kept)

    def near(shards):
        def pair(g, carry):
            c0 = pl.multiple_of(g * PAIR, PAIR)
            for s in shards:
                r0 = row_of(s, 0, shard)
                span = pl.ds(r0, ROW_BLOCK)
                o, sums = attend(
                    q_c[span, pl.ds(c0, PAIR)],
                    kv_ext[pl.ds(r0, window), pl.ds(c0, PAIR)],
                    kv_ext[pl.ds(r0, window), pl.ds(c0 + col_count, PAIR)],
                    bias_near[span],
                )
                o_near[g, span, :] = o
                keep_sums(lse_near, span, g, sums)
            return carry

        lax.fori_loop(0, group_count, pair, 0)

    my_share = pl.ds(pl.multiple_of(sp * share, share), share)

    def back_total(seg):
        return bulk(ret.at[seg, pl.ds(0, others)], back_send.at[seg], back_recv.at[seg])

    def lback_total(seg):
        return bulk(ret_lse.at[seg, pl.ds(0, sp_size - 1)], lback_send.at[seg], lback_recv.at[seg])

    def class_attend(seg, groups=None):
        span = slice(seg * shard, (seg + 1) * shard)

        def block(g):
            c0 = pl.multiple_of(g * PAIR, PAIR)
            o, sums = attend(
                cls_recv[span, pl.ds(c0 + Q * col_count, PAIR)],
                cls_recv[:, pl.ds(c0 + K * col_count, PAIR)],
                cls_recv[:, pl.ds(c0 + V * col_count, PAIR)],
                bias_class[span],
            )
            cls_o[span, pl.ds(c0, PAIR)] = o.astype(bf16)
            keep_sums(cls_lse, span, g, sums)

        def two(i, carry):
            block(2 * i)
            block(2 * i + 1)
            return carry

        if groups is None:
            lax.fori_loop(0, group_count // 2, two, 0)
        else:
            for g in groups:
                block(g)

    def send_back(seg, groups):
        cols = slice(groups[0] * PAIR, (groups[-1] + 1) * PAIR)
        for off in offsets:
            dest = (sp + off) % sp_size
            part = pl.ds(pl.multiple_of(seg * shard + dest * share, share), share)
            remote(
                cls_o.at[part, cols], ret.at[seg, my_share, cols],
                back_send.at[seg], back_recv.at[seg], sp=dest,
            ).start()
        mine = pl.ds(pl.multiple_of(seg * shard + sp * share, share), share)
        ret[seg, my_share, cols] = cls_o[mine, cols]

    def send_sums(seg):
        span = slice(seg * shard, (seg + 1) * shard)
        lse_out[seg] = exchange_blocks(jnp.transpose(cls_lse[span])[:head_count])[:, None, :]
        for off in offsets:
            dest = (sp + off) % sp_size
            remote(
                lse_out.at[seg, dest], ret_lse.at[seg, sp], lback_send.at[seg], lback_recv.at[seg],
                sp=dest,
            ).start()
        ret_lse[seg, sp] = lse_out[seg, sp]
        waits.append(back_total(seg))
        waits.append(lback_total(seg))

    head_lane = lax.broadcasted_iota(jnp.int32, (head_count, PAIR), 1)

    head_row = lax.broadcasted_iota(jnp.int32, (head_count, PAIR), 0)

    def exchange_blocks(x):
        out = x
        for k in range(1, head_count):
            moved = pltpu.roll(pltpu.roll(x, k * share, 1), head_count - k, 0)
            out = jnp.where(head_lane // share == (head_row + k) % head_count, moved, out)
        return out

    def gather_rows(ref, seg):
        return jnp.concatenate([ref[pl.ds(row_of(s, a, c), c)] for s, a, c in spans[seg]], axis=0)

    def combine(seg):
        lback_total(seg).wait_recv()
        flat = exchange_blocks(ret_lse[seg][:, 0, :])
        tall = jnp.transpose(
            jnp.concatenate([flat, jnp.zeros((PAIR - head_count, PAIR), f32)], axis=0)
        )
        for r in range(sp_size):
            lse_f[pl.ds(r, share, stride=sp_size), :] = tall[r * share : (r + 1) * share]
        back_total(seg).wait_recv()
        for g in range(group_count):
            for r in range(sp_size):
                ret_f[g, pl.ds(r, share, stride=sp_size), :] = ret[
                    seg, r * share : (r + 1) * share, g * PAIR : (g + 1) * PAIR
                ].astype(f32)
        la = gather_rows(lse_near, seg)
        lb = lse_f[...]
        peak = jnp.maximum(la, lb)
        ea = jnp.exp(la - peak)
        eb = jnp.exp(lb - peak)
        total = ea + eb
        logw = jnp.transpose(peak + jnp.log(total))[:head_count]
        if seg < 2:
            logw_ref[:, pl.ds(row_of(*spans[seg][0]), shard)] = logw
        else:
            logw_far[seg - 2] = logw
        ea = ea / total
        eb = eb / total
        for g in range(group_count):
            wa = jnp.where(first_head, ea[:, 2 * g : 2 * g + 1], ea[:, 2 * g + 1 : 2 * g + 2])
            wb = jnp.where(first_head, eb[:, 2 * g : 2 * g + 1], eb[:, 2 * g + 1 : 2 * g + 2])
            mixed = wa * gather_rows(o_near.at[g], seg) + wb * ret_f[g]
            att[seg, :, g * PAIR : (g + 1) * PAIR] = mixed.astype(bf16)

    width = wo.shape[1] // OUT_SPLITS

    def product(seg, n):
        return jnp.dot(
            att[seg], wo[:, n * width : (n + 1) * width], preferred_element_type=f32
        ).astype(bf16)

    exch, cross = {}, {}

    def relay(k, n):
        exch[k, n].wait_recv()
        cross_out[k, n] = (keep_b[k, n].astype(f32) + part_in[k, n].astype(f32)).astype(bf16)
        cross[k, n] = remote(
            cross_out.at[k, n], cross_in.at[k, n], cr_send.at[k], cr_recv.at[k, n], tp=far_same
        )
        cross[k, n].start()

    def out_far(k):
        for n in range(OUT_SPLITS):
            both = product(2 + k, n)
            part_out[k, n] = both[piece:]
            exch[k, n] = remote(
                part_out.at[k, n], part_in.at[k, n], ex_send.at[k], ex_recv.at[k, n], tp=partner
            )
            exch[k, n].start()
            keep_b[k, n] = both[:piece]
            if n:
                relay(k, n - 1)
        relay(k, OUT_SPLITS - 1)
        waits.append(bulk(part_out.at[k], ex_send.at[k], ex_recv.at[k, 0]))
        waits.append(bulk(cross_out.at[k], cr_send.at[k], cr_recv.at[k, 0]))

    lse_near[...] = jnp.zeros_like(lse_near)
    cls_lse[...] = jnp.zeros_like(cls_lse)
    halo_early.wait_recv()
    near((far_same, far_other))
    all_groups = range(group_count)
    low_groups, high_groups = all_groups[: group_count // 2], all_groups[group_count // 2 :]
    gathered(0, 1, 4, 5)
    scatter(6)
    class_attend(2, low_groups)
    send_back(2, low_groups)
    class_attend(2, high_groups)
    send_back(2, high_groups)
    send_sums(2)
    gathered(6)
    class_attend(3)
    load_out.wait()
    combine(2)
    send_back(3, all_groups)
    send_sums(3)
    out_far(0)
    gathered(2)
    class_attend(0)
    combine(3)
    out_far(1)
    send_back(0, all_groups)
    send_sums(0)
    halo_late = edge(1 - chip, 1)
    gathered(3)
    class_attend(1)
    send_back(1, all_groups)
    send_sums(1)
    first_half = head_lane < piece
    swap = [pltpu.roll(logw_far[k], piece, 1) for k in range(SPLITS)]
    logw_ref[:, pl.ds(row_of(far_same, 0, shard), shard)] = jnp.where(
        first_half, logw_far[0], swap[1]
    )
    logw_ref[:, pl.ds(row_of(far_other, 0, shard), shard)] = jnp.where(
        first_half, swap[0], logw_far[1]
    )
    halo_late.wait_recv()
    near((tp, partner))
    combine(1)
    for n in range(OUT_SPLITS):
        own_out[n] = product(1, n)
        remote(own_out.at[n], own_in.at[n], ox_send.at[0], ox_recv.at[0], tp=partner).start()
    own_total = bulk(own_in, ox_send.at[0], ox_recv.at[0])
    waits.append(own_total)
    combine(0)
    for n in range(OUT_SPLITS):
        keep_d[n] = product(0, n).astype(f32)
    own_total.wait_recv()
    for n in range(OUT_SPLITS):
        keep_d[n] = keep_d[n] + own_in[n].astype(f32)
    for k in range(SPLITS):
        for n in range(OUT_SPLITS):
            cross[k, n].wait_recv()
            out_ref[k * piece : (k + 1) * piece, n * width : (n + 1) * width] = (
                keep_d[n, k * piece : (k + 1) * piece] + cross_in[k, n].astype(f32)
            ).astype(bf16)

    for item in waits:
        item.wait_send()


def fused(sp_size, tp_size, tokens_in, w_query, w_key, w_value, w_out):
    shard, depth = tokens_in.shape
    col_count = w_query.shape[1]
    rows = shard * tp_size
    groups = col_count // PAIR
    heads = col_count // HEAD_DIM
    share = shard // sp_size
    piece = shard // SPLITS
    wide = w_out.shape[1]
    width = wide // OUT_SPLITS
    half = HEAD_DIM // 2
    freq = 1.0 / ROTARY_BASE ** (np.arange(half) / half)
    freq = np.tile(freq, PAIR // half)
    start = np.concatenate([np.arange(rows), np.arange(sp_size) * rows])
    angle = start[:, None] * freq[None, :]
    cosine, sine = np.cos(angle), np.sin(angle)
    table = jnp.asarray(np.stack([cosine, sine, cosine, sine]).astype(np.float32))
    f32, bf16 = jnp.float32, jnp.bfloat16
    V_, DMA = pltpu.VMEM, pltpu.SemaphoreType.DMA
    window = ROW_BLOCK + 2 * SIDE_SPAN
    scratch = [
        V_((tp_size, shard, depth), bf16),
        V_((3, depth, col_count), bf16),
        V_((col_count, wide), bf16),
        V_((2,) + table.shape[1:], f32),
        V_((rows, PAIR), f32),
        V_((rows, PAIR), f32),
        V_((rows, col_count), bf16),
        V_((rows + 2 * SIDE_SPAN, 2 * col_count), bf16),
        V_((3 * groups, rows, PAIR), f32),
        V_((sp_size, SEGMENTS * share, 3 * col_count), bf16),
        V_((rows, 3 * col_count), bf16),
        V_((rows, window), f32),
        V_((rows, rows), f32),
        V_((groups, rows, PAIR), f32),
        V_((rows, PAIR), f32),
        V_((rows, col_count), bf16),
        V_((rows, PAIR), f32),
        V_((SEGMENTS, sp_size, 1, PAIR), f32),
        V_((SEGMENTS, shard, col_count), bf16),
        V_((SEGMENTS, sp_size, 1, PAIR), f32),
        V_((groups, shard, PAIR), f32),
        V_((shard, PAIR), f32),
        V_((SPLITS, heads, PAIR), f32),
        V_((SEGMENTS, shard, col_count), bf16),
        V_((SPLITS, OUT_SPLITS, piece, width), bf16),
        V_((SPLITS, OUT_SPLITS, piece, width), bf16),
        V_((SPLITS, OUT_SPLITS, piece, width), bf16),
        V_((SPLITS, OUT_SPLITS, piece, width), bf16),
        V_((SPLITS, OUT_SPLITS, piece, width), bf16),
        V_((OUT_SPLITS, shard, width), f32),
        V_((OUT_SPLITS, shard, width), bf16),
        V_((OUT_SPLITS, shard, width), bf16),
        DMA((6,)),
        DMA((1,)), DMA((1,)),
        DMA((SPLITS,)), DMA((SPLITS,)),
        DMA((SPLITS,)), DMA((SPLITS,)),
        DMA((len(UNITS),)), DMA((len(UNITS),)),
        DMA((2,)), DMA((2,)),
        DMA((SEGMENTS,)), DMA((SEGMENTS,)),
        DMA((SEGMENTS,)), DMA((SEGMENTS,)),
        DMA((SPLITS,)), DMA((SPLITS, OUT_SPLITS)),
        DMA((SPLITS,)), DMA((SPLITS, OUT_SPLITS)),
        DMA((1,)), DMA((1,)),
    ]
    hbm = pl.BlockSpec(memory_space=pltpu.HBM)
    vmem = pl.BlockSpec(memory_space=pltpu.VMEM)
    return pl.pallas_call(
        functools.partial(class_kernel, sp_size, tp_size, col_count),
        out_shape=(
            jax.ShapeDtypeStruct((shard, wide), bf16),
            jax.ShapeDtypeStruct((heads, rows), f32),
        ),
        in_specs=[hbm] * 6,
        out_specs=(vmem, vmem),
        scratch_shapes=scratch,
        compiler_params=pltpu.CompilerParams(
            collective_id=0, has_side_effects=True, vmem_limit_bytes=VMEM_GRANT
        ),
        name="dilated_layer",
    )(tokens_in, w_query, w_key, w_value, w_out, table)


VMEM_GRANT = 52 * 1024 * 1024


def solution(mesh):
    in_specs = (P(("sp", "tp"), None), P(None, "tp"), P(None, "tp"), P(None, "tp"), P("tp", None))
    out_specs = (P(("sp", "tp"), None), P("tp", "sp"))
    sp_size, tp_size = mesh.shape["sp"], mesh.shape["tp"]

    def body(*args):
        shard = args[0].shape[0]
        whole_class = (
            MIDDLE_DILATION % sp_size == 0
            and WIDEST_DILATION % sp_size == 0
            and tp_size == 2 * SPLITS
            and shard == ROW_BLOCK
            and shard == 16 * sp_size
            and args[1].shape[1] == sp_size * HEAD_DIM
        )
        if whole_class:
            return fused(sp_size, tp_size, *args)
        return per_device(*args)

    return jax.shard_map(body, mesh=mesh, in_specs=in_specs, out_specs=out_specs, check_vma=False)
```

```python
import functools

import jax
import jax.numpy as jnp
import numpy as np
from jax import lax
from jax.experimental import pallas as pl
from jax.experimental.pallas import tpu as pltpu
from jax.sharding import PartitionSpec as P

HEAD_DIM = 64
SIDE_SPAN = 64
MIDDLE_DILATION = 8
WIDEST_DILATION = 64


ROTARY_BASE = 500000.0
NEGATIVE = -1e30


def shifted(block, axis, distance):
    devices = range(lax.axis_size(axis))
    route = [(i - distance, i) for i in devices if i - distance in devices]
    return lax.ppermute(block, axis, route)


def rotate(block, positions):
    half_size = block.shape[-1] // 2
    freq = 1.0 / ROTARY_BASE ** (jnp.arange(half_size, dtype=jnp.float32) / half_size)
    angle = positions[:, None] * freq[None, :]
    cosine = jnp.cos(angle)[:, None, :]
    sine = jnp.sin(angle)[:, None, :]
    front = block[..., :half_size]
    back = block[..., half_size:]
    return jnp.concatenate([front * cosine - back * sine, back * cosine + front * sine], axis=-1)


def pattern_attend(query, keys, values, lead_rows, dilation_step, low_row, high_row):
    rows_total, head_count, head_size = query.shape
    class_len = rows_total // dilation_step
    first_class = lead_rows // dilation_step - SIDE_SPAN
    class_q = query.reshape(class_len, dilation_step, head_count, head_size)
    class_k = keys.reshape(keys.shape[0] // dilation_step, dilation_step, head_count, head_size)
    class_v = values.reshape(values.shape[0] // dilation_step, dilation_step, head_count, head_size)
    sub_k = class_k[first_class : first_class + class_len + 2 * SIDE_SPAN]
    sub_v = class_v[first_class : first_class + class_len + 2 * SIDE_SPAN]
    if class_len <= SIDE_SPAN:
        block_len = class_len
        block_count = 1
        win_k = sub_k[None]
        win_v = sub_v[None]
        blocks_q = class_q[None]
    else:
        block_len = SIDE_SPAN
        block_count = class_len // SIDE_SPAN
        part_k = sub_k.reshape(block_count + 2, SIDE_SPAN, dilation_step, head_count, head_size)
        part_v = sub_v.reshape(block_count + 2, SIDE_SPAN, dilation_step, head_count, head_size)
        win_k = jnp.concatenate([part_k[:-2], part_k[1:-1], part_k[2:]], axis=1)
        win_v = jnp.concatenate([part_v[:-2], part_v[1:-1], part_v[2:]], axis=1)
        blocks_q = class_q.reshape(block_count, SIDE_SPAN, dilation_step, head_count, head_size)
    width = block_len + 2 * SIDE_SPAN
    scores = jnp.einsum("nasht,nksht->nshak", blocks_q, win_k, preferred_element_type=jnp.float32)
    scores = scores * head_size ** (-0.5)
    q_index = jnp.arange(block_len, dtype=jnp.int32)
    k_index = jnp.arange(width, dtype=jnp.int32)
    b_index = jnp.arange(block_count, dtype=jnp.int32)
    s_index = jnp.arange(dilation_step, dtype=jnp.int32)
    in_band = jnp.abs(k_index[None, :] - SIDE_SPAN - q_index[:, None]) <= SIDE_SPAN
    key_position = (
        (first_class + b_index[:, None] * block_len + k_index[None, :]) * dilation_step
    )[:, None, :] + s_index[None, :, None]
    is_valid = (key_position >= low_row) & (key_position < high_row)
    keep_mask = in_band[None, None, None] & is_valid[:, :, None, None, :]
    scores = jnp.where(keep_mask, scores, NEGATIVE)
    maxima = jnp.max(scores, axis=-1, keepdims=True)
    expo = jnp.exp(scores - maxima)
    totals = jnp.sum(expo, axis=-1)
    numerator = jnp.einsum(
        "nshak,nksht->nasht", expo.astype(jnp.bfloat16), win_v, preferred_element_type=jnp.float32
    )
    totals_t = jnp.transpose(totals, (0, 3, 1, 2))
    result = (
        (numerator / totals_t[..., None])
        .astype(jnp.bfloat16)
        .reshape(rows_total, head_count, head_size)
    )
    log_sum = jnp.transpose(maxima[..., 0] + jnp.log(totals), (0, 3, 1, 2)).reshape(
        rows_total, head_count
    )
    return (result, log_sum)


def combine(results):
    sums = jnp.stack([item[1] for item in results], axis=0)
    peak = jnp.max(sums, axis=0)
    share = jnp.exp(sums - peak[None])
    weight_sum = share[0] + share[1] + share[2]
    accum = share[0][..., None] * results[0][0].astype(jnp.float32)
    accum = accum + share[1][..., None] * results[1][0].astype(jnp.float32)
    accum = accum + share[2][..., None] * results[2][0].astype(jnp.float32)
    attended = (accum / weight_sum[..., None]).astype(jnp.bfloat16)
    return (attended, peak + jnp.log(weight_sum))


def per_device(tokens_in, w_query, w_key, w_value, w_out):
    col_count = w_query.shape[1]
    head_count = col_count // HEAD_DIM
    piece = lax.all_gather(tokens_in, "tp", axis=0, tiled=True)
    projected = jnp.concatenate(
        [
            jnp.dot(piece, w_query, preferred_element_type=jnp.float32),
            jnp.dot(piece, w_key, preferred_element_type=jnp.float32),
            jnp.dot(piece, w_value, preferred_element_type=jnp.float32),
        ],
        axis=1,
    )
    rows_total = projected.shape[0]
    sp_size = lax.axis_size("sp")
    sp_place = lax.axis_index("sp")
    positions = (sp_place * rows_total + jnp.arange(rows_total, dtype=jnp.int32)).astype(
        jnp.float32
    )
    shape3 = (rows_total, head_count, HEAD_DIM)
    query = rotate(projected[:, :col_count].reshape(shape3), positions).astype(jnp.bfloat16)
    keys = rotate(projected[:, col_count : 2 * col_count].reshape(shape3), positions).astype(
        jnp.bfloat16
    )
    values = projected[:, 2 * col_count :].astype(jnp.bfloat16).reshape(shape3)
    per_device_span = -(-(SIDE_SPAN * MIDDLE_DILATION) // rows_total)
    earlier_k = []
    earlier_v = []
    before_k, before_v = shifted((keys, values), "sp", 1)
    after_k, after_v = shifted((keys, values), "sp", -1)
    earlier_k.insert(0, before_k)
    earlier_v.insert(0, before_v)
    later_k = [after_k]
    later_v = [after_v]
    key_buf = jnp.concatenate(earlier_k + [keys] + later_k, axis=0)
    value_buf = jnp.concatenate(earlier_v + [values] + later_v, axis=0)
    lead_rows = per_device_span * rows_total
    low_row = lead_rows - sp_place * rows_total
    key_buf, value_buf, lead_rows, low_row, high_row = (
        key_buf,
        value_buf,
        lead_rows,
        low_row,
        low_row + sp_size * rows_total,
    )
    results = [
        pattern_attend(query, key_buf, value_buf, lead_rows, dilation_step, low_row, high_row)
        for dilation_step in (1, MIDDLE_DILATION)
    ]
    class_stride = WIDEST_DILATION // sp_size
    border_extent = SIDE_SPAN * class_stride
    class_shape = (rows_total // sp_size, sp_size, head_count, HEAD_DIM)
    parts = (
        lax.all_to_all(query.reshape(class_shape), "sp", split_axis=1, concat_axis=0, tiled=True),
        lax.all_to_all(keys.reshape(class_shape), "sp", split_axis=1, concat_axis=0, tiled=True),
        lax.all_to_all(values.reshape(class_shape), "sp", split_axis=1, concat_axis=0, tiled=True),
    )
    item_heads = parts[0].shape[2]
    flat = [item.reshape(rows_total, item_heads, HEAD_DIM) for item in parts]
    pad_k = jnp.pad(flat[1], ((border_extent, border_extent), (0, 0), (0, 0)))
    pad_v = jnp.pad(flat[2], ((border_extent, border_extent), (0, 0), (0, 0)))
    result, log_sum = pattern_attend(
        flat[0],
        pad_k,
        pad_v,
        border_extent,
        class_stride,
        border_extent,
        border_extent + rows_total,
    )
    result_back = lax.all_to_all(
        result.reshape(rows_total, 1, item_heads, HEAD_DIM),
        "sp",
        split_axis=0,
        concat_axis=1,
        tiled=True,
    )
    sum_back = lax.all_to_all(
        log_sum.reshape(rows_total, 1, item_heads), "sp", split_axis=0, concat_axis=1, tiled=True
    )
    results.append((result_back.reshape(shape3), sum_back.reshape(rows_total, head_count)))
    attended, log_weight = combine(results)
    flat_out = attended.reshape(rows_total, col_count)
    mixed = lax.psum_scatter(
        jnp.dot(flat_out, w_out, preferred_element_type=jnp.float32).astype(jnp.bfloat16),
        "tp",
        scatter_dimension=0,
        tiled=True,
    )
    return (mixed, jnp.transpose(log_weight, (1, 0)))


MESH_ID = pl.DeviceIdType.MESH
PAIR = 2 * HEAD_DIM
ROW_BLOCK = 128
SPLITS = 2
OUT_SPLITS = 4
SEGMENTS = 4
K, V, Q = 0, 1, 2
UNITS = ((0, (K, V)), (1, (K, V)), (0, (Q,)), (1, (Q,)), (2, (K, V, Q)), (3, (K, V)), (3, (Q,)))


def class_kernel(
    sp_size, tp_size, col_count,
    x_hbm, wq_hbm, wk_hbm, wv_hbm, wo_hbm, table_hbm,
    out_ref, logw_ref,
    x_all, w_all, wo, table, cos_t, sin_t, q_c, kv_ext, pf, cls_send, cls_recv,
    bias_near, bias_class, o_near, lse_near, cls_o, cls_lse, lse_out, ret, ret_lse, ret_f, lse_f, logw_far,
    lead_o, lead_top, lead_total, att, part_out, part_in, cross_out, cross_in, keep_b, keep_d, own_out, own_in,
    load_sem, own_send, own_recv, far_send, far_recv, fwd_send, fwd_recv,
    a2a_send, a2a_recv, halo_send, halo_recv, back_send, back_recv, lback_send, lback_recv,
    ex_send, ex_recv, cr_send, cr_recv, ox_send, ox_recv,
):
    sp = lax.axis_index("sp")
    tp = lax.axis_index("tp")
    chip = tp // 2
    core = tp % 2
    partner = chip * 2 + (1 - core)
    far_same = (1 - chip) * 2 + core
    far_other = (1 - chip) * 2 + (1 - core)
    shard = x_hbm.shape[0]
    rows = shard * tp_size
    piece = shard // SPLITS
    group_count = col_count // PAIR
    head_count = col_count // HEAD_DIM
    share = shard // sp_size
    f32, bf16 = jnp.float32, jnp.bfloat16

    offsets = sorted(range(1, sp_size), key=lambda off: (abs(off - sp_size // 2), off))

    spans = (
        ((tp, 0, shard),),
        ((partner, 0, shard),),
        ((far_same, 0, piece), (far_other, 0, piece)),
        ((far_same, piece, piece), (far_other, piece, piece)),
    )

    def row_of(s, a, c):
        return pl.multiple_of(s * shard + a, c)

    load_table = pltpu.make_async_copy(table_hbm.at[0:2], table, load_sem.at[0])
    load_x = pltpu.make_async_copy(x_hbm, x_all.at[tp], load_sem.at[1])
    load_w = [
        pltpu.make_async_copy(w, w_all.at[n], load_sem.at[2 + n])
        for n, w in enumerate((wk_hbm, wv_hbm, wq_hbm))
    ]
    load_out = pltpu.make_async_copy(wo_hbm, wo, load_sem.at[5])
    load_x.start()
    load_table.start()
    for item in load_w:
        item.start()

    barrier = pltpu.get_barrier_semaphore()
    pl.semaphore_signal(barrier, inc=1, device_id={"tp": partner}, device_id_type=MESH_ID)
    pl.semaphore_signal(barrier, inc=1, device_id={"tp": far_same}, device_id_type=MESH_ID)
    for off in offsets:
        pl.semaphore_signal(
            barrier, inc=1, device_id={"sp": (sp + off) % sp_size}, device_id_type=MESH_ID
        )
    pl.semaphore_wait(barrier, 2 + (sp_size - 1))

    def remote(src, dst, send, recv, **where):
        return pltpu.make_async_remote_copy(
            src_ref=src, dst_ref=dst, send_sem=send, recv_sem=recv,
            device_id=where, device_id_type=MESH_ID,
        )

    waits = []

    def launch(item):
        item.start()
        waits.append(item)
        return item

    far = []
    for k in range(SPLITS):
        span = pl.ds(k * piece, piece)
        far.append(
            launch(
                remote(
                    x_hbm.at[span], x_all.at[tp, span], far_send.at[k], far_recv.at[k], tp=far_same
                )
            )
        )
    own = launch(remote(x_hbm, x_all.at[tp], own_send.at[0], own_recv.at[0], tp=partner))
    load_out.start()

    lane = lax.broadcasted_iota(jnp.int32, (1, PAIR), 1)
    front = lane % HEAD_DIM < HEAD_DIM // 2
    first_head = lane < HEAD_DIM
    sign = jnp.where(front, -1.0, 1.0).astype(f32)
    load_table.wait()
    base_cos = table[0, pl.ds(rows + sp, 1), :]
    base_sin = table[1, pl.ds(rows + sp, 1), :]
    for r0 in range(0, rows, ROW_BLOCK):
        lc = table[0, r0 : r0 + ROW_BLOCK]
        ls = table[1, r0 : r0 + ROW_BLOCK]
        cos_t[r0 : r0 + ROW_BLOCK] = lc * base_cos - ls * base_sin
        sin_t[r0 : r0 + ROW_BLOCK] = (ls * base_cos + lc * base_sin) * sign

    window = ROW_BLOCK + 2 * SIDE_SPAN
    mid_step = MIDDLE_DILATION // sp_size
    wide_step = WIDEST_DILATION // sp_size
    per_source = rows // sp_size
    half_share = share // 2

    def place_of(seg, index):
        source = index // share
        j = index % share
        if seg < 2:
            inner = spans[seg][0][0] * share + j
        else:
            inner = jnp.where(
                j < half_share,
                far_same * share + (seg - 2) * half_share + j,
                far_other * share + (seg - 3) * half_share + j,
            )
        return source * per_source + inner

    def build_bias():
        near_i = lax.broadcasted_iota(jnp.int32, (ROW_BLOCK, window), 0)
        near_j = lax.broadcasted_iota(jnp.int32, (ROW_BLOCK, window), 1)
        near_band = jnp.abs(near_j - SIDE_SPAN - near_i) <= SIDE_SPAN
        for r0 in range(0, rows, ROW_BLOCK):
            key_pos = sp * rows + r0 + near_j - SIDE_SPAN
            good = near_band & (key_pos >= 0) & (key_pos < sp_size * rows)
            bias_near[r0 : r0 + ROW_BLOCK] = jnp.where(good, 0.0, NEGATIVE)
        for a in range(SEGMENTS):
            q_place = place_of(a, lax.broadcasted_iota(jnp.int32, (ROW_BLOCK, 1), 0))
            for b in range(SEGMENTS):
                k_place = place_of(b, lax.broadcasted_iota(jnp.int32, (1, ROW_BLOCK), 1))
                gap = jnp.abs(q_place - k_place)
                mid = (gap % mid_step == 0) & (gap <= SIDE_SPAN * mid_step)
                wide = (gap % wide_step == 0) & (gap <= SIDE_SPAN * wide_step)
                bias_class[
                    a * ROW_BLOCK : (a + 1) * ROW_BLOCK, b * ROW_BLOCK : (b + 1) * ROW_BLOCK
                ] = jnp.where(
                    mid & wide, float(np.log(2.0)), jnp.where(mid | wide, 0.0, NEGATIVE)
                )

    def turn(x, cos, sin):
        swapped = jnp.where(
            front, pltpu.roll(x, PAIR - HEAD_DIM // 2, 1), pltpu.roll(x, HEAD_DIM // 2, 1)
        )
        return x * cos + swapped * sin

    def project(seg, n):
        if len(spans[seg]) == 1:
            left = x_all[spans[seg][0][0]]
        else:
            left = jnp.concatenate([x_all[s, pl.ds(a, c)] for s, a, c in spans[seg]], axis=0)
        full = jnp.dot(left, w_all[n], preferred_element_type=f32)
        at = 0
        for s, a, c in spans[seg]:
            r0 = row_of(s, a, c)
            if n != V:
                cos = cos_t[pl.ds(r0, c)]
                sin = sin_t[pl.ds(r0, c)]
            for g in range(group_count):
                part = full[at : at + c, g * PAIR : (g + 1) * PAIR]
                if n != V:
                    part = turn(part, cos, sin)
                pf[n * group_count + g, seg * shard + at : seg * shard + at + c, :] = part
                low = part.astype(bf16)
                if n == Q:
                    q_c[pl.ds(r0, c), g * PAIR : (g + 1) * PAIR] = low
                else:
                    kv_ext[
                        pl.ds(r0 + SIDE_SPAN, c),
                        n * col_count + g * PAIR : n * col_count + (g + 1) * PAIR,
                    ] = low
            at += c

    def bulk(ref, send, recv):
        return remote(ref, ref, send, recv, tp=partner)

    others = (sp_size - 1) * share

    def a2a_total(unit):
        seg, names = UNITS[unit]
        cols = slice(names[0] * col_count, (names[-1] + 1) * col_count)
        return bulk(
            cls_recv.at[pl.ds(seg * shard, others), cols], a2a_send.at[unit], a2a_recv.at[unit]
        )

    def scatter(unit):
        seg, names = UNITS[unit]
        span = slice(seg * share, (seg + 1) * share)
        cols = slice(names[0] * col_count, (names[-1] + 1) * col_count)

        def one(r, carry):
            for g in range(names[0] * group_count, (names[-1] + 1) * group_count):
                cls_send[r, span, g * PAIR : (g + 1) * PAIR] = pf[
                    g, pl.ds(seg * shard + r, share, stride=sp_size), :
                ].astype(bf16)
            return carry

        lax.fori_loop(0, sp_size, one, 0)
        mine = pl.ds(pl.multiple_of(seg * shard + sp * share, share), share)
        for off in offsets:
            dest = (sp + off) % sp_size
            remote(
                cls_send.at[dest, span, cols], cls_recv.at[mine, cols],
                a2a_send.at[unit], a2a_recv.at[unit], sp=dest,
            ).start()
        waits.append(a2a_total(unit))
        cls_recv[mine, cols] = cls_send[sp, span, cols]

    def gathered(*units):
        for unit in units:
            a2a_total(unit).wait_recv()

    def edge(which, n):
        src = pl.multiple_of(SIDE_SPAN + which * (rows - SIDE_SPAN), SIDE_SPAN)
        dst = pl.multiple_of((1 - which) * (rows + SIDE_SPAN), SIDE_SPAN)
        return launch(
            remote(
                kv_ext.at[pl.ds(src, SIDE_SPAN)], kv_ext.at[pl.ds(dst, SIDE_SPAN)],
                halo_send.at[n], halo_recv.at[n], sp=(sp + sp_size - 1 + 2 * which) % sp_size,
            )
        )

    load_x.wait()
    load_w[K].wait()
    project(0, K)
    load_w[V].wait()
    project(0, V)
    scatter(0)
    own.wait_recv()
    project(1, K)
    project(1, V)
    scatter(1)
    halo_early = edge(chip, 0)
    load_w[Q].wait()
    project(0, Q)
    scatter(2)
    project(1, Q)

    fwd = []
    for k in range(SPLITS):
        span = pl.ds(k * piece, piece)
        far[k].wait_recv()
        fwd.append(
            launch(
                remote(
                    x_all.at[far_same, span], x_all.at[far_same, span],
                    fwd_send.at[k], fwd_recv.at[k], tp=partner,
                )
            )
        )
        if k == 0:
            build_bias()
        fwd[k].wait_recv()
        project(2 + k, K)
        project(2 + k, V)
        if k == 0:
            project(2, Q)
            scatter(4)
        else:
            scatter(5)
            project(3, Q)

    lane_wide = lax.broadcasted_iota(jnp.int32, (ROW_BLOCK, PAIR), 1)
    scale = HEAD_DIM ** (-0.5)

    def pair_scores(query, keys):
        q = query.astype(f32) * scale
        both = jnp.concatenate(
            [jnp.where(first_head, q, 0.0), jnp.where(first_head, 0.0, q)], axis=0
        ).astype(bf16)
        s = lax.dot_general(both, keys, (((1,), (1,)), ((), ())), preferred_element_type=f32)
        return s[: query.shape[0]], s[query.shape[0] :]

    def pair_product(e, values):
        o = jnp.dot(
            jnp.concatenate(e, axis=0).astype(bf16), values, preferred_element_type=f32
        )
        return o[: e[0].shape[0]], o[e[0].shape[0] :]

    def soften(query, keys, bias):
        e, tops, totals = [], [], []
        for s in pair_scores(query, keys):
            s = s + bias
            top = jnp.max(s, axis=1, keepdims=True)
            part = jnp.exp(s - top)
            e.append(part)
            tops.append(top)
            totals.append(jnp.sum(part, axis=1, keepdims=True))
        return e, tops, totals

    def attend(query, keys, values, bias):
        e, tops, totals = soften(query, keys, bias)
        o = pair_product(e, values)
        sums = [top + jnp.log(total) for top, total in zip(tops, totals)]
        return jnp.where(first_head, o[0] / totals[0], o[1] / totals[1]), sums

    def keep_sums(ref, span, g, sums):
        kept = ref[span]
        kept = jnp.where(lane_wide == 2 * g, sums[0], kept)
        ref[span] = jnp.where(lane_wide == 2 * g + 1, sums[1], kept)

    def near(shards):
        def pair(g, carry):
            c0 = pl.multiple_of(g * PAIR, PAIR)
            for s in shards:
                r0 = row_of(s, 0, shard)
                span = pl.ds(r0, ROW_BLOCK)
                o, sums = attend(
                    q_c[span, pl.ds(c0, PAIR)],
                    kv_ext[pl.ds(r0, window), pl.ds(c0, PAIR)],
                    kv_ext[pl.ds(r0, window), pl.ds(c0 + col_count, PAIR)],
                    bias_near[span],
                )
                o_near[g, span, :] = o
                keep_sums(lse_near, span, g, sums)
            return carry

        lax.fori_loop(0, group_count, pair, 0)

    my_share = pl.ds(pl.multiple_of(sp * share, share), share)

    def back_total(seg):
        return bulk(ret.at[seg, pl.ds(0, others)], back_send.at[seg], back_recv.at[seg])

    def lback_total(seg):
        return bulk(ret_lse.at[seg, pl.ds(0, sp_size - 1)], lback_send.at[seg], lback_recv.at[seg])

    def class_attend(seg):
        span = slice(seg * shard, (seg + 1) * shard)

        def block(g):
            c0 = pl.multiple_of(g * PAIR, PAIR)
            o, sums = attend(
                cls_recv[span, pl.ds(c0 + Q * col_count, PAIR)],
                cls_recv[:, pl.ds(c0 + K * col_count, PAIR)],
                cls_recv[:, pl.ds(c0 + V * col_count, PAIR)],
                bias_class[span],
            )
            cls_o[span, pl.ds(c0, PAIR)] = o.astype(bf16)
            keep_sums(cls_lse, span, g, sums)

        def two(i, carry):
            block(2 * i)
            block(2 * i + 1)
            return carry

        lax.fori_loop(0, group_count // 2, two, 0)

    lead_keys = (SEGMENTS - 1) * shard

    def class_lead(seg):
        span = slice(seg * shard, (seg + 1) * shard)

        def one(g, carry):
            c0 = pl.multiple_of(g * PAIR, PAIR)
            e, tops, totals = soften(
                cls_recv[span, pl.ds(c0 + Q * col_count, PAIR)],
                cls_recv[:lead_keys, pl.ds(c0 + K * col_count, PAIR)],
                bias_class[span, :lead_keys],
            )
            o = pair_product(e, cls_recv[:lead_keys, pl.ds(c0 + V * col_count, PAIR)])
            lead_o[g] = jnp.where(first_head, o[0], o[1])
            for half in range(2):
                lead_top[2 * g + half] = jnp.broadcast_to(tops[half], (shard, PAIR))
                lead_total[2 * g + half] = jnp.broadcast_to(totals[half], (shard, PAIR))
            return carry

        def two(i, carry):
            one(2 * i, carry)
            return one(2 * i + 1, carry)

        lax.fori_loop(0, group_count // 2, two, 0)

    def class_rest(seg, groups):
        span = slice(seg * shard, (seg + 1) * shard)
        for g in groups:
            cols = [slice(n * col_count + g * PAIR, n * col_count + (g + 1) * PAIR) for n in (K, V, Q)]
            parts = pair_scores(cls_recv[span, cols[Q]], cls_recv[lead_keys:, cols[K]])
            e, sums, decays, totals = [], [], [], []
            for half, s in enumerate(parts):
                s = s + bias_class[span, lead_keys:]
                old = lead_top[2 * g + half]
                top = jnp.maximum(old, jnp.max(s, axis=1, keepdims=True))
                part = jnp.exp(s - top)
                decay = jnp.exp(old - top)
                total = lead_total[2 * g + half] * decay + jnp.sum(part, axis=1, keepdims=True)
                e.append(part)
                decays.append(decay)
                totals.append(total)
                sums.append(top + jnp.log(total))
            o = pair_product(e, cls_recv[lead_keys:, cols[V]])
            o = jnp.where(first_head, o[0], o[1])
            decay = jnp.where(first_head, decays[0], decays[1])
            total = jnp.where(first_head, totals[0], totals[1])
            cls_o[span, g * PAIR : (g + 1) * PAIR] = ((lead_o[g] * decay + o) / total).astype(bf16)
            keep_sums(cls_lse, span, g, sums)

    def send_back(seg, groups):
        cols = slice(groups[0] * PAIR, (groups[-1] + 1) * PAIR)
        for off in offsets:
            dest = (sp + off) % sp_size
            part = pl.ds(pl.multiple_of(seg * shard + dest * share, share), share)
            remote(
                cls_o.at[part, cols], ret.at[seg, my_share, cols],
                back_send.at[seg], back_recv.at[seg], sp=dest,
            ).start()
        mine = pl.ds(pl.multiple_of(seg * shard + sp * share, share), share)
        ret[seg, my_share, cols] = cls_o[mine, cols]

    def send_sums(seg):
        span = slice(seg * shard, (seg + 1) * shard)
        lse_out[seg] = exchange_blocks(jnp.transpose(cls_lse[span])[:head_count])[:, None, :]
        for off in offsets:
            dest = (sp + off) % sp_size
            remote(
                lse_out.at[seg, dest], ret_lse.at[seg, sp], lback_send.at[seg], lback_recv.at[seg],
                sp=dest,
            ).start()
        ret_lse[seg, sp] = lse_out[seg, sp]
        waits.append(back_total(seg))
        waits.append(lback_total(seg))

    head_lane = lax.broadcasted_iota(jnp.int32, (head_count, PAIR), 1)

    head_row = lax.broadcasted_iota(jnp.int32, (head_count, PAIR), 0)

    def exchange_blocks(x):
        out = x
        for k in range(1, head_count):
            moved = pltpu.roll(pltpu.roll(x, k * share, 1), head_count - k, 0)
            out = jnp.where(head_lane // share == (head_row + k) % head_count, moved, out)
        return out

    def gather_rows(ref, seg):
        return jnp.concatenate([ref[pl.ds(row_of(s, a, c), c)] for s, a, c in spans[seg]], axis=0)

    def combine(seg):
        lback_total(seg).wait_recv()
        flat = exchange_blocks(ret_lse[seg][:, 0, :])
        tall = jnp.transpose(
            jnp.concatenate([flat, jnp.zeros((PAIR - head_count, PAIR), f32)], axis=0)
        )
        for r in range(sp_size):
            lse_f[pl.ds(r, share, stride=sp_size), :] = tall[r * share : (r + 1) * share]
        back_total(seg).wait_recv()
        for g in range(group_count):
            for r in range(sp_size):
                ret_f[g, pl.ds(r, share, stride=sp_size), :] = ret[
                    seg, r * share : (r + 1) * share, g * PAIR : (g + 1) * PAIR
                ].astype(f32)
        la = gather_rows(lse_near, seg)
        lb = lse_f[...]
        peak = jnp.maximum(la, lb)
        ea = jnp.exp(la - peak)
        eb = jnp.exp(lb - peak)
        total = ea + eb
        logw = jnp.transpose(peak + jnp.log(total))[:head_count]
        if seg < 2:
            logw_ref[:, pl.ds(row_of(*spans[seg][0]), shard)] = logw
        else:
            logw_far[seg - 2] = logw
        ea = ea / total
        eb = eb / total
        for g in range(group_count):
            wa = jnp.where(first_head, ea[:, 2 * g : 2 * g + 1], ea[:, 2 * g + 1 : 2 * g + 2])
            wb = jnp.where(first_head, eb[:, 2 * g : 2 * g + 1], eb[:, 2 * g + 1 : 2 * g + 2])
            mixed = wa * gather_rows(o_near.at[g], seg) + wb * ret_f[g]
            att[seg, :, g * PAIR : (g + 1) * PAIR] = mixed.astype(bf16)

    width = wo.shape[1] // OUT_SPLITS

    def product(seg, n):
        return jnp.dot(
            att[seg], wo[:, n * width : (n + 1) * width], preferred_element_type=f32
        ).astype(bf16)

    exch, cross = {}, {}

    def relay(k, n):
        exch[k, n].wait_recv()
        cross_out[k, n] = (keep_b[k, n].astype(f32) + part_in[k, n].astype(f32)).astype(bf16)
        cross[k, n] = remote(
            cross_out.at[k, n], cross_in.at[k, n], cr_send.at[k], cr_recv.at[k, n], tp=far_same
        )
        cross[k, n].start()

    def out_far(k):
        for n in range(OUT_SPLITS):
            both = product(2 + k, n)
            part_out[k, n] = both[piece:]
            exch[k, n] = remote(
                part_out.at[k, n], part_in.at[k, n], ex_send.at[k], ex_recv.at[k, n], tp=partner
            )
            exch[k, n].start()
            keep_b[k, n] = both[:piece]
            if n:
                relay(k, n - 1)
        relay(k, OUT_SPLITS - 1)
        waits.append(bulk(part_out.at[k], ex_send.at[k], ex_recv.at[k, 0]))
        waits.append(bulk(cross_out.at[k], cr_send.at[k], cr_recv.at[k, 0]))

    lse_near[...] = jnp.zeros_like(lse_near)
    cls_lse[...] = jnp.zeros_like(cls_lse)
    halo_early.wait_recv()
    near((far_same, far_other))
    all_groups = range(group_count)
    low_groups, high_groups = all_groups[: group_count // 2], all_groups[group_count // 2 :]
    gathered(0, 1, 4)
    class_lead(2)
    all_groups = range(group_count)
    low_groups, high_groups = all_groups[: group_count // 2], all_groups[group_count // 2 :]
    gathered(5)
    class_rest(2, low_groups)
    send_back(2, low_groups)
    class_rest(2, high_groups)
    send_back(2, high_groups)
    send_sums(2)
    gathered(2)
    class_attend(0)
    scatter(6)
    load_out.wait()
    combine(2)
    scatter(3)
    halo_late = edge(1 - chip, 1)
    out_far(0)
    gathered(6)
    class_attend(3)
    send_back(3, all_groups)
    send_sums(3)
    gathered(3)
    class_attend(1)
    halo_late.wait_recv()
    near((tp, partner))
    send_back(1, all_groups)
    send_sums(1)
    combine(3)
    send_back(0, all_groups)
    send_sums(0)
    out_far(1)
    first_half = head_lane < piece
    swap = [pltpu.roll(logw_far[k], piece, 1) for k in range(SPLITS)]
    logw_ref[:, pl.ds(row_of(far_same, 0, shard), shard)] = jnp.where(
        first_half, logw_far[0], swap[1]
    )
    logw_ref[:, pl.ds(row_of(far_other, 0, shard), shard)] = jnp.where(
        first_half, swap[0], logw_far[1]
    )
    combine(1)
    for n in range(OUT_SPLITS):
        own_out[n] = product(1, n)
        remote(own_out.at[n], own_in.at[n], ox_send.at[0], ox_recv.at[0], tp=partner).start()
    own_total = bulk(own_in, ox_send.at[0], ox_recv.at[0])
    waits.append(own_total)
    combine(0)
    for n in range(OUT_SPLITS):
        keep_d[n] = product(0, n).astype(f32)
    own_total.wait_recv()
    for n in range(OUT_SPLITS):
        keep_d[n] = keep_d[n] + own_in[n].astype(f32)
    for k in range(SPLITS):
        for n in range(OUT_SPLITS):
            cross[k, n].wait_recv()
            out_ref[k * piece : (k + 1) * piece, n * width : (n + 1) * width] = (
                keep_d[n, k * piece : (k + 1) * piece] + cross_in[k, n].astype(f32)
            ).astype(bf16)

    for item in waits:
        item.wait_send()


def fused(sp_size, tp_size, tokens_in, w_query, w_key, w_value, w_out):
    shard, depth = tokens_in.shape
    col_count = w_query.shape[1]
    rows = shard * tp_size
    groups = col_count // PAIR
    heads = col_count // HEAD_DIM
    share = shard // sp_size
    piece = shard // SPLITS
    wide = w_out.shape[1]
    width = wide // OUT_SPLITS
    half = HEAD_DIM // 2
    freq = 1.0 / ROTARY_BASE ** (np.arange(half) / half)
    freq = np.tile(freq, PAIR // half)
    start = np.concatenate([np.arange(rows), np.arange(sp_size) * rows])
    angle = start[:, None] * freq[None, :]
    cosine, sine = np.cos(angle), np.sin(angle)
    table = jnp.asarray(np.stack([cosine, sine, cosine, sine]).astype(np.float32))
    f32, bf16 = jnp.float32, jnp.bfloat16
    V_, DMA = pltpu.VMEM, pltpu.SemaphoreType.DMA
    window = ROW_BLOCK + 2 * SIDE_SPAN
    scratch = [
        V_((tp_size, shard, depth), bf16),
        V_((3, depth, col_count), bf16),
        V_((col_count, wide), bf16),
        V_((2,) + table.shape[1:], f32),
        V_((rows, PAIR), f32),
        V_((rows, PAIR), f32),
        V_((rows, col_count), bf16),
        V_((rows + 2 * SIDE_SPAN, 2 * col_count), bf16),
        V_((3 * groups, rows, PAIR), f32),
        V_((sp_size, SEGMENTS * share, 3 * col_count), bf16),
        V_((rows, 3 * col_count), bf16),
        V_((rows, window), f32),
        V_((rows, rows), f32),
        V_((groups, rows, PAIR), f32),
        V_((rows, PAIR), f32),
        V_((rows, col_count), bf16),
        V_((rows, PAIR), f32),
        V_((SEGMENTS, sp_size, 1, PAIR), f32),
        V_((SEGMENTS, shard, col_count), bf16),
        V_((SEGMENTS, sp_size, 1, PAIR), f32),
        V_((groups, shard, PAIR), f32),
        V_((shard, PAIR), f32),
        V_((SPLITS, heads, PAIR), f32),
        V_((groups, shard, PAIR), f32),
        V_((heads, shard, PAIR), f32),
        V_((heads, shard, PAIR), f32),
        V_((SEGMENTS, shard, col_count), bf16),
        V_((SPLITS, OUT_SPLITS, piece, width), bf16),
        V_((SPLITS, OUT_SPLITS, piece, width), bf16),
        V_((SPLITS, OUT_SPLITS, piece, width), bf16),
        V_((SPLITS, OUT_SPLITS, piece, width), bf16),
        V_((SPLITS, OUT_SPLITS, piece, width), bf16),
        V_((OUT_SPLITS, shard, width), f32),
        V_((OUT_SPLITS, shard, width), bf16),
        V_((OUT_SPLITS, shard, width), bf16),
        DMA((6,)),
        DMA((1,)), DMA((1,)),
        DMA((SPLITS,)), DMA((SPLITS,)),
        DMA((SPLITS,)), DMA((SPLITS,)),
        DMA((len(UNITS),)), DMA((len(UNITS),)),
        DMA((2,)), DMA((2,)),
        DMA((SEGMENTS,)), DMA((SEGMENTS,)),
        DMA((SEGMENTS,)), DMA((SEGMENTS,)),
        DMA((SPLITS,)), DMA((SPLITS, OUT_SPLITS)),
        DMA((SPLITS,)), DMA((SPLITS, OUT_SPLITS)),
        DMA((1,)), DMA((1,)),
    ]
    hbm = pl.BlockSpec(memory_space=pltpu.HBM)
    vmem = pl.BlockSpec(memory_space=pltpu.VMEM)
    return pl.pallas_call(
        functools.partial(class_kernel, sp_size, tp_size, col_count),
        out_shape=(
            jax.ShapeDtypeStruct((shard, wide), bf16),
            jax.ShapeDtypeStruct((heads, rows), f32),
        ),
        in_specs=[hbm] * 6,
        out_specs=(vmem, vmem),
        scratch_shapes=scratch,
        compiler_params=pltpu.CompilerParams(
            collective_id=0, has_side_effects=True, vmem_limit_bytes=VMEM_GRANT
        ),
        name="dilated_layer",
    )(tokens_in, w_query, w_key, w_value, w_out, table)


VMEM_GRANT = 52 * 1024 * 1024


def solution(mesh):
    in_specs = (P(("sp", "tp"), None), P(None, "tp"), P(None, "tp"), P(None, "tp"), P("tp", None))
    out_specs = (P(("sp", "tp"), None), P("tp", "sp"))
    sp_size, tp_size = mesh.shape["sp"], mesh.shape["tp"]

    def body(*args):
        shard = args[0].shape[0]
        whole_class = (
            MIDDLE_DILATION % sp_size == 0
            and WIDEST_DILATION % sp_size == 0
            and tp_size == 2 * SPLITS
            and shard == ROW_BLOCK
            and shard == 16 * sp_size
            and args[1].shape[1] == sp_size * HEAD_DIM
        )
        if whole_class:
            return fused(sp_size, tp_size, *args)
        return per_device(*args)

    return jax.shard_map(body, mesh=mesh, in_specs=in_specs, out_specs=out_specs, check_vma=False)
```

```python
import functools

import jax
import jax.numpy as jnp
import numpy as np
from jax import lax
from jax.experimental import pallas as pl
from jax.experimental.pallas import tpu as pltpu
from jax.sharding import PartitionSpec as P

HEAD_DIM = 64
SIDE_SPAN = 64
MIDDLE_DILATION = 8
WIDEST_DILATION = 64


ROTARY_BASE = 500000.0
NEGATIVE = -1e30


def shifted(block, axis, distance):
    devices = range(lax.axis_size(axis))
    route = [(i - distance, i) for i in devices if i - distance in devices]
    return lax.ppermute(block, axis, route)


def rotate(block, positions):
    half_size = block.shape[-1] // 2
    freq = 1.0 / ROTARY_BASE ** (jnp.arange(half_size, dtype=jnp.float32) / half_size)
    angle = positions[:, None] * freq[None, :]
    cosine = jnp.cos(angle)[:, None, :]
    sine = jnp.sin(angle)[:, None, :]
    front = block[..., :half_size]
    back = block[..., half_size:]
    return jnp.concatenate([front * cosine - back * sine, back * cosine + front * sine], axis=-1)


def pattern_attend(query, keys, values, lead_rows, dilation_step, low_row, high_row):
    rows_total, head_count, head_size = query.shape
    class_len = rows_total // dilation_step
    first_class = lead_rows // dilation_step - SIDE_SPAN
    class_q = query.reshape(class_len, dilation_step, head_count, head_size)
    class_k = keys.reshape(keys.shape[0] // dilation_step, dilation_step, head_count, head_size)
    class_v = values.reshape(values.shape[0] // dilation_step, dilation_step, head_count, head_size)
    sub_k = class_k[first_class : first_class + class_len + 2 * SIDE_SPAN]
    sub_v = class_v[first_class : first_class + class_len + 2 * SIDE_SPAN]
    if class_len <= SIDE_SPAN:
        block_len = class_len
        block_count = 1
        win_k = sub_k[None]
        win_v = sub_v[None]
        blocks_q = class_q[None]
    else:
        block_len = SIDE_SPAN
        block_count = class_len // SIDE_SPAN
        part_k = sub_k.reshape(block_count + 2, SIDE_SPAN, dilation_step, head_count, head_size)
        part_v = sub_v.reshape(block_count + 2, SIDE_SPAN, dilation_step, head_count, head_size)
        win_k = jnp.concatenate([part_k[:-2], part_k[1:-1], part_k[2:]], axis=1)
        win_v = jnp.concatenate([part_v[:-2], part_v[1:-1], part_v[2:]], axis=1)
        blocks_q = class_q.reshape(block_count, SIDE_SPAN, dilation_step, head_count, head_size)
    width = block_len + 2 * SIDE_SPAN
    scores = jnp.einsum("nasht,nksht->nshak", blocks_q, win_k, preferred_element_type=jnp.float32)
    scores = scores * head_size ** (-0.5)
    q_index = jnp.arange(block_len, dtype=jnp.int32)
    k_index = jnp.arange(width, dtype=jnp.int32)
    b_index = jnp.arange(block_count, dtype=jnp.int32)
    s_index = jnp.arange(dilation_step, dtype=jnp.int32)
    in_band = jnp.abs(k_index[None, :] - SIDE_SPAN - q_index[:, None]) <= SIDE_SPAN
    key_position = (
        (first_class + b_index[:, None] * block_len + k_index[None, :]) * dilation_step
    )[:, None, :] + s_index[None, :, None]
    is_valid = (key_position >= low_row) & (key_position < high_row)
    keep_mask = in_band[None, None, None] & is_valid[:, :, None, None, :]
    scores = jnp.where(keep_mask, scores, NEGATIVE)
    maxima = jnp.max(scores, axis=-1, keepdims=True)
    expo = jnp.exp(scores - maxima)
    totals = jnp.sum(expo, axis=-1)
    numerator = jnp.einsum(
        "nshak,nksht->nasht", expo.astype(jnp.bfloat16), win_v, preferred_element_type=jnp.float32
    )
    totals_t = jnp.transpose(totals, (0, 3, 1, 2))
    result = (
        (numerator / totals_t[..., None])
        .astype(jnp.bfloat16)
        .reshape(rows_total, head_count, head_size)
    )
    log_sum = jnp.transpose(maxima[..., 0] + jnp.log(totals), (0, 3, 1, 2)).reshape(
        rows_total, head_count
    )
    return (result, log_sum)


def combine(results):
    sums = jnp.stack([item[1] for item in results], axis=0)
    peak = jnp.max(sums, axis=0)
    share = jnp.exp(sums - peak[None])
    weight_sum = share[0] + share[1] + share[2]
    accum = share[0][..., None] * results[0][0].astype(jnp.float32)
    accum = accum + share[1][..., None] * results[1][0].astype(jnp.float32)
    accum = accum + share[2][..., None] * results[2][0].astype(jnp.float32)
    attended = (accum / weight_sum[..., None]).astype(jnp.bfloat16)
    return (attended, peak + jnp.log(weight_sum))


def per_device(tokens_in, w_query, w_key, w_value, w_out):
    col_count = w_query.shape[1]
    head_count = col_count // HEAD_DIM
    piece = lax.all_gather(tokens_in, "tp", axis=0, tiled=True)
    projected = jnp.concatenate(
        [
            jnp.dot(piece, w_query, preferred_element_type=jnp.float32),
            jnp.dot(piece, w_key, preferred_element_type=jnp.float32),
            jnp.dot(piece, w_value, preferred_element_type=jnp.float32),
        ],
        axis=1,
    )
    rows_total = projected.shape[0]
    sp_size = lax.axis_size("sp")
    sp_place = lax.axis_index("sp")
    positions = (sp_place * rows_total + jnp.arange(rows_total, dtype=jnp.int32)).astype(
        jnp.float32
    )
    shape3 = (rows_total, head_count, HEAD_DIM)
    query = rotate(projected[:, :col_count].reshape(shape3), positions).astype(jnp.bfloat16)
    keys = rotate(projected[:, col_count : 2 * col_count].reshape(shape3), positions).astype(
        jnp.bfloat16
    )
    values = projected[:, 2 * col_count :].astype(jnp.bfloat16).reshape(shape3)
    per_device_span = -(-(SIDE_SPAN * MIDDLE_DILATION) // rows_total)
    earlier_k = []
    earlier_v = []
    before_k, before_v = shifted((keys, values), "sp", 1)
    after_k, after_v = shifted((keys, values), "sp", -1)
    earlier_k.insert(0, before_k)
    earlier_v.insert(0, before_v)
    later_k = [after_k]
    later_v = [after_v]
    key_buf = jnp.concatenate(earlier_k + [keys] + later_k, axis=0)
    value_buf = jnp.concatenate(earlier_v + [values] + later_v, axis=0)
    lead_rows = per_device_span * rows_total
    low_row = lead_rows - sp_place * rows_total
    key_buf, value_buf, lead_rows, low_row, high_row = (
        key_buf,
        value_buf,
        lead_rows,
        low_row,
        low_row + sp_size * rows_total,
    )
    results = [
        pattern_attend(query, key_buf, value_buf, lead_rows, dilation_step, low_row, high_row)
        for dilation_step in (1, MIDDLE_DILATION)
    ]
    class_stride = WIDEST_DILATION // sp_size
    border_extent = SIDE_SPAN * class_stride
    class_shape = (rows_total // sp_size, sp_size, head_count, HEAD_DIM)
    parts = (
        lax.all_to_all(query.reshape(class_shape), "sp", split_axis=1, concat_axis=0, tiled=True),
        lax.all_to_all(keys.reshape(class_shape), "sp", split_axis=1, concat_axis=0, tiled=True),
        lax.all_to_all(values.reshape(class_shape), "sp", split_axis=1, concat_axis=0, tiled=True),
    )
    item_heads = parts[0].shape[2]
    flat = [item.reshape(rows_total, item_heads, HEAD_DIM) for item in parts]
    pad_k = jnp.pad(flat[1], ((border_extent, border_extent), (0, 0), (0, 0)))
    pad_v = jnp.pad(flat[2], ((border_extent, border_extent), (0, 0), (0, 0)))
    result, log_sum = pattern_attend(
        flat[0],
        pad_k,
        pad_v,
        border_extent,
        class_stride,
        border_extent,
        border_extent + rows_total,
    )
    result_back = lax.all_to_all(
        result.reshape(rows_total, 1, item_heads, HEAD_DIM),
        "sp",
        split_axis=0,
        concat_axis=1,
        tiled=True,
    )
    sum_back = lax.all_to_all(
        log_sum.reshape(rows_total, 1, item_heads), "sp", split_axis=0, concat_axis=1, tiled=True
    )
    results.append((result_back.reshape(shape3), sum_back.reshape(rows_total, head_count)))
    attended, log_weight = combine(results)
    flat_out = attended.reshape(rows_total, col_count)
    mixed = lax.psum_scatter(
        jnp.dot(flat_out, w_out, preferred_element_type=jnp.float32).astype(jnp.bfloat16),
        "tp",
        scatter_dimension=0,
        tiled=True,
    )
    return (mixed, jnp.transpose(log_weight, (1, 0)))


MESH_ID = pl.DeviceIdType.MESH
PAIR = 2 * HEAD_DIM
ROW_BLOCK = 128
SPLITS = 2
OUT_SPLITS = 4
SEGMENTS = 4
K, V, Q = 0, 1, 2
UNITS = ((0, (K, V)), (1, (K, V)), (0, (Q,)), (1, (Q,)), (2, (K, V, Q)), (3, (K, V)), (3, (Q,)))


def class_kernel(
    sp_size, tp_size, col_count,
    x_hbm, wq_hbm, wk_hbm, wv_hbm, wo_hbm, table_hbm,
    out_ref, logw_ref,
    x_all, w_all, wo, table, cos_t, sin_t, q_c, kv_ext, pf, cls_send, cls_recv,
    bias_near, bias_class, o_near, lse_near, cls_o, cls_lse, lse_out, ret, ret_lse, ret_f, lse_f, logw_far,
    lead_o, lead_top, lead_total, att, part_out, part_in, cross_out, cross_in, keep_b, keep_d, own_out, own_in,
    load_sem, own_send, own_recv, far_send, far_recv, fwd_send, fwd_recv,
    a2a_send, a2a_recv, halo_send, halo_recv, back_send, back_recv, lback_send, lback_recv,
    ex_send, ex_recv, cr_send, cr_recv, ox_send, ox_recv,
):
    sp = lax.axis_index("sp")
    tp = lax.axis_index("tp")
    chip = tp // 2
    core = tp % 2
    partner = chip * 2 + (1 - core)
    far_same = (1 - chip) * 2 + core
    far_other = (1 - chip) * 2 + (1 - core)
    shard = x_hbm.shape[0]
    rows = shard * tp_size
    piece = shard // SPLITS
    group_count = col_count // PAIR
    head_count = col_count // HEAD_DIM
    share = shard // sp_size
    f32, bf16 = jnp.float32, jnp.bfloat16

    offsets = sorted(range(1, sp_size), key=lambda off: (abs(off - sp_size // 2), off))

    spans = (
        ((tp, 0, shard),),
        ((partner, 0, shard),),
        ((far_same, 0, piece), (far_other, 0, piece)),
        ((far_same, piece, piece), (far_other, piece, piece)),
    )

    def row_of(s, a, c):
        return pl.multiple_of(s * shard + a, c)

    load_table = pltpu.make_async_copy(table_hbm.at[0:2], table, load_sem.at[0])
    load_x = pltpu.make_async_copy(x_hbm, x_all.at[tp], load_sem.at[1])
    load_w = [
        pltpu.make_async_copy(w, w_all.at[n], load_sem.at[2 + n])
        for n, w in enumerate((wk_hbm, wv_hbm, wq_hbm))
    ]
    load_out = pltpu.make_async_copy(wo_hbm, wo, load_sem.at[5])
    load_x.start()
    load_table.start()
    for item in load_w:
        item.start()

    barrier = pltpu.get_barrier_semaphore()
    pl.semaphore_signal(barrier, inc=1, device_id={"tp": partner}, device_id_type=MESH_ID)
    pl.semaphore_signal(barrier, inc=1, device_id={"tp": far_same}, device_id_type=MESH_ID)
    for off in offsets:
        pl.semaphore_signal(
            barrier, inc=1, device_id={"sp": (sp + off) % sp_size}, device_id_type=MESH_ID
        )
    pl.semaphore_wait(barrier, 2 + (sp_size - 1))

    def remote(src, dst, send, recv, **where):
        return pltpu.make_async_remote_copy(
            src_ref=src, dst_ref=dst, send_sem=send, recv_sem=recv,
            device_id=where, device_id_type=MESH_ID,
        )

    waits = []

    def launch(item):
        item.start()
        waits.append(item)
        return item

    far = []
    for k in range(SPLITS):
        span = pl.ds(k * piece, piece)
        far.append(
            launch(
                remote(
                    x_hbm.at[span], x_all.at[tp, span], far_send.at[k], far_recv.at[k], tp=far_same
                )
            )
        )
    own = launch(remote(x_hbm, x_all.at[tp], own_send.at[0], own_recv.at[0], tp=partner))
    load_out.start()

    lane = lax.broadcasted_iota(jnp.int32, (1, PAIR), 1)
    front = lane % HEAD_DIM < HEAD_DIM // 2
    first_head = lane < HEAD_DIM
    sign = jnp.where(front, -1.0, 1.0).astype(f32)
    load_table.wait()
    base_cos = table[0, pl.ds(rows + sp, 1), :]
    base_sin = table[1, pl.ds(rows + sp, 1), :]
    for r0 in range(0, rows, ROW_BLOCK):
        lc = table[0, r0 : r0 + ROW_BLOCK]
        ls = table[1, r0 : r0 + ROW_BLOCK]
        cos_t[r0 : r0 + ROW_BLOCK] = lc * base_cos - ls * base_sin
        sin_t[r0 : r0 + ROW_BLOCK] = (ls * base_cos + lc * base_sin) * sign

    window = ROW_BLOCK + 2 * SIDE_SPAN
    mid_step = MIDDLE_DILATION // sp_size
    wide_step = WIDEST_DILATION // sp_size
    per_source = rows // sp_size
    half_share = share // 2

    def place_of(seg, index):
        source = index // share
        j = index % share
        if seg < 2:
            inner = spans[seg][0][0] * share + j
        else:
            inner = jnp.where(
                j < half_share,
                far_same * share + (seg - 2) * half_share + j,
                far_other * share + (seg - 3) * half_share + j,
            )
        return source * per_source + inner

    def build_bias():
        near_i = lax.broadcasted_iota(jnp.int32, (ROW_BLOCK, window), 0)
        near_j = lax.broadcasted_iota(jnp.int32, (ROW_BLOCK, window), 1)
        near_band = jnp.abs(near_j - SIDE_SPAN - near_i) <= SIDE_SPAN
        for r0 in range(0, rows, ROW_BLOCK):
            key_pos = sp * rows + r0 + near_j - SIDE_SPAN
            good = near_band & (key_pos >= 0) & (key_pos < sp_size * rows)
            bias_near[r0 : r0 + ROW_BLOCK] = jnp.where(good, 0.0, NEGATIVE)
        for a in range(SEGMENTS):
            q_place = place_of(a, lax.broadcasted_iota(jnp.int32, (ROW_BLOCK, 1), 0))
            for b in range(SEGMENTS):
                k_place = place_of(b, lax.broadcasted_iota(jnp.int32, (1, ROW_BLOCK), 1))
                gap = jnp.abs(q_place - k_place)
                mid = (gap % mid_step == 0) & (gap <= SIDE_SPAN * mid_step)
                wide = (gap % wide_step == 0) & (gap <= SIDE_SPAN * wide_step)
                bias_class[
                    a * ROW_BLOCK : (a + 1) * ROW_BLOCK, b * ROW_BLOCK : (b + 1) * ROW_BLOCK
                ] = jnp.where(
                    mid & wide, float(np.log(2.0)), jnp.where(mid | wide, 0.0, NEGATIVE)
                )

    def turn(x, cos, sin):
        swapped = jnp.where(
            front, pltpu.roll(x, PAIR - HEAD_DIM // 2, 1), pltpu.roll(x, HEAD_DIM // 2, 1)
        )
        return x * cos + swapped * sin

    def project(seg, n):
        if len(spans[seg]) == 1:
            left = x_all[spans[seg][0][0]]
        else:
            left = jnp.concatenate([x_all[s, pl.ds(a, c)] for s, a, c in spans[seg]], axis=0)
        full = jnp.dot(left, w_all[n], preferred_element_type=f32)
        at = 0
        for s, a, c in spans[seg]:
            r0 = row_of(s, a, c)
            if n != V:
                cos = cos_t[pl.ds(r0, c)]
                sin = sin_t[pl.ds(r0, c)]
            for g in range(group_count):
                part = full[at : at + c, g * PAIR : (g + 1) * PAIR]
                if n != V:
                    part = turn(part, cos, sin)
                pf[n * group_count + g, seg * shard + at : seg * shard + at + c, :] = part
                low = part.astype(bf16)
                if n == Q:
                    q_c[pl.ds(r0, c), g * PAIR : (g + 1) * PAIR] = low
                else:
                    kv_ext[
                        pl.ds(r0 + SIDE_SPAN, c),
                        n * col_count + g * PAIR : n * col_count + (g + 1) * PAIR,
                    ] = low
            at += c

    def bulk(ref, send, recv):
        return remote(ref, ref, send, recv, tp=partner)

    others = (sp_size - 1) * share

    def a2a_total(unit):
        seg, names = UNITS[unit]
        cols = slice(names[0] * col_count, (names[-1] + 1) * col_count)
        return bulk(
            cls_recv.at[pl.ds(seg * shard, others), cols], a2a_send.at[unit], a2a_recv.at[unit]
        )

    def scatter(unit):
        seg, names = UNITS[unit]
        span = slice(seg * share, (seg + 1) * share)
        cols = slice(names[0] * col_count, (names[-1] + 1) * col_count)

        def one(r, carry):
            for g in range(names[0] * group_count, (names[-1] + 1) * group_count):
                cls_send[r, span, g * PAIR : (g + 1) * PAIR] = pf[
                    g, pl.ds(seg * shard + r, share, stride=sp_size), :
                ].astype(bf16)
            return carry

        lax.fori_loop(0, sp_size, one, 0)
        mine = pl.ds(pl.multiple_of(seg * shard + sp * share, share), share)
        for off in offsets:
            dest = (sp + off) % sp_size
            remote(
                cls_send.at[dest, span, cols], cls_recv.at[mine, cols],
                a2a_send.at[unit], a2a_recv.at[unit], sp=dest,
            ).start()
        waits.append(a2a_total(unit))
        cls_recv[mine, cols] = cls_send[sp, span, cols]

    def gathered(*units):
        for unit in units:
            a2a_total(unit).wait_recv()

    def edge(which, n):
        src = pl.multiple_of(SIDE_SPAN + which * (rows - SIDE_SPAN), SIDE_SPAN)
        dst = pl.multiple_of((1 - which) * (rows + SIDE_SPAN), SIDE_SPAN)
        return launch(
            remote(
                kv_ext.at[pl.ds(src, SIDE_SPAN)], kv_ext.at[pl.ds(dst, SIDE_SPAN)],
                halo_send.at[n], halo_recv.at[n], sp=(sp + sp_size - 1 + 2 * which) % sp_size,
            )
        )

    load_x.wait()
    load_w[K].wait()
    project(0, K)
    load_w[V].wait()
    project(0, V)
    scatter(0)
    own.wait_recv()
    project(1, K)
    project(1, V)
    scatter(1)
    halo_early = edge(chip, 0)
    load_w[Q].wait()
    project(1, Q)
    scatter(3)
    project(0, Q)

    fwd = []
    for k in range(SPLITS):
        span = pl.ds(k * piece, piece)
        far[k].wait_recv()
        fwd.append(
            launch(
                remote(
                    x_all.at[far_same, span], x_all.at[far_same, span],
                    fwd_send.at[k], fwd_recv.at[k], tp=partner,
                )
            )
        )
        if k == 0:
            build_bias()
        fwd[k].wait_recv()
        project(2 + k, K)
        project(2 + k, V)
        if k == 0:
            project(2, Q)
            scatter(4)
        else:
            scatter(5)
            project(3, Q)

    lane_wide = lax.broadcasted_iota(jnp.int32, (ROW_BLOCK, PAIR), 1)
    scale = HEAD_DIM ** (-0.5)

    def pair_scores(query, keys):
        q = query.astype(f32) * scale
        both = jnp.concatenate(
            [jnp.where(first_head, q, 0.0), jnp.where(first_head, 0.0, q)], axis=0
        ).astype(bf16)
        s = lax.dot_general(both, keys, (((1,), (1,)), ((), ())), preferred_element_type=f32)
        return s[: query.shape[0]], s[query.shape[0] :]

    def pair_product(e, values):
        o = jnp.dot(
            jnp.concatenate(e, axis=0).astype(bf16), values, preferred_element_type=f32
        )
        return o[: e[0].shape[0]], o[e[0].shape[0] :]

    def soften(query, keys, bias):
        e, tops, totals = [], [], []
        for s in pair_scores(query, keys):
            s = s + bias
            top = jnp.max(s, axis=1, keepdims=True)
            part = jnp.exp(s - top)
            e.append(part)
            tops.append(top)
            totals.append(jnp.sum(part, axis=1, keepdims=True))
        return e, tops, totals

    def attend(query, keys, values, bias):
        e, tops, totals = soften(query, keys, bias)
        o = pair_product(e, values)
        sums = [top + jnp.log(total) for top, total in zip(tops, totals)]
        return jnp.where(first_head, o[0] / totals[0], o[1] / totals[1]), sums

    def keep_sums(ref, span, g, sums):
        kept = ref[span]
        kept = jnp.where(lane_wide == 2 * g, sums[0], kept)
        ref[span] = jnp.where(lane_wide == 2 * g + 1, sums[1], kept)

    def near(shards):
        def pair(g, carry):
            c0 = pl.multiple_of(g * PAIR, PAIR)
            for s in shards:
                r0 = row_of(s, 0, shard)
                span = pl.ds(r0, ROW_BLOCK)
                o, sums = attend(
                    q_c[span, pl.ds(c0, PAIR)],
                    kv_ext[pl.ds(r0, window), pl.ds(c0, PAIR)],
                    kv_ext[pl.ds(r0, window), pl.ds(c0 + col_count, PAIR)],
                    bias_near[span],
                )
                o_near[g, span, :] = o
                keep_sums(lse_near, span, g, sums)
            return carry

        lax.fori_loop(0, group_count, pair, 0)

    my_share = pl.ds(pl.multiple_of(sp * share, share), share)

    def back_total(seg):
        return bulk(ret.at[seg, pl.ds(0, others)], back_send.at[seg], back_recv.at[seg])

    def lback_total(seg):
        return bulk(ret_lse.at[seg, pl.ds(0, sp_size - 1)], lback_send.at[seg], lback_recv.at[seg])

    def class_attend(seg, groups=None):
        span = slice(seg * shard, (seg + 1) * shard)

        def block(g):
            c0 = pl.multiple_of(g * PAIR, PAIR)
            o, sums = attend(
                cls_recv[span, pl.ds(c0 + Q * col_count, PAIR)],
                cls_recv[:, pl.ds(c0 + K * col_count, PAIR)],
                cls_recv[:, pl.ds(c0 + V * col_count, PAIR)],
                bias_class[span],
            )
            cls_o[span, pl.ds(c0, PAIR)] = o.astype(bf16)
            keep_sums(cls_lse, span, g, sums)

        def two(i, carry):
            block(2 * i)
            block(2 * i + 1)
            return carry

        if groups is None:
            lax.fori_loop(0, group_count // 2, two, 0)
        else:
            for g in groups:
                block(g)

    lead_keys = (SEGMENTS - 1) * shard

    def class_lead(seg):
        span = slice(seg * shard, (seg + 1) * shard)

        def one(g, carry):
            c0 = pl.multiple_of(g * PAIR, PAIR)
            e, tops, totals = soften(
                cls_recv[span, pl.ds(c0 + Q * col_count, PAIR)],
                cls_recv[:lead_keys, pl.ds(c0 + K * col_count, PAIR)],
                bias_class[span, :lead_keys],
            )
            o = pair_product(e, cls_recv[:lead_keys, pl.ds(c0 + V * col_count, PAIR)])
            lead_o[g] = jnp.where(first_head, o[0], o[1])
            for half in range(2):
                lead_top[2 * g + half] = jnp.broadcast_to(tops[half], (shard, PAIR))
                lead_total[2 * g + half] = jnp.broadcast_to(totals[half], (shard, PAIR))
            return carry

        def two(i, carry):
            one(2 * i, carry)
            return one(2 * i + 1, carry)

        lax.fori_loop(0, group_count // 2, two, 0)

    def class_rest(seg, groups):
        span = slice(seg * shard, (seg + 1) * shard)
        for g in groups:
            cols = [slice(n * col_count + g * PAIR, n * col_count + (g + 1) * PAIR) for n in (K, V, Q)]
            parts = pair_scores(cls_recv[span, cols[Q]], cls_recv[lead_keys:, cols[K]])
            e, sums, decays, totals = [], [], [], []
            for half, s in enumerate(parts):
                s = s + bias_class[span, lead_keys:]
                old = lead_top[2 * g + half]
                top = jnp.maximum(old, jnp.max(s, axis=1, keepdims=True))
                part = jnp.exp(s - top)
                decay = jnp.exp(old - top)
                total = lead_total[2 * g + half] * decay + jnp.sum(part, axis=1, keepdims=True)
                e.append(part)
                decays.append(decay)
                totals.append(total)
                sums.append(top + jnp.log(total))
            o = pair_product(e, cls_recv[lead_keys:, cols[V]])
            o = jnp.where(first_head, o[0], o[1])
            decay = jnp.where(first_head, decays[0], decays[1])
            total = jnp.where(first_head, totals[0], totals[1])
            cls_o[span, g * PAIR : (g + 1) * PAIR] = ((lead_o[g] * decay + o) / total).astype(bf16)
            keep_sums(cls_lse, span, g, sums)

    def send_back(seg, groups):
        cols = slice(groups[0] * PAIR, (groups[-1] + 1) * PAIR)
        for off in offsets:
            dest = (sp + off) % sp_size
            part = pl.ds(pl.multiple_of(seg * shard + dest * share, share), share)
            remote(
                cls_o.at[part, cols], ret.at[seg, my_share, cols],
                back_send.at[seg], back_recv.at[seg], sp=dest,
            ).start()
        mine = pl.ds(pl.multiple_of(seg * shard + sp * share, share), share)
        ret[seg, my_share, cols] = cls_o[mine, cols]

    def send_sums(seg):
        span = slice(seg * shard, (seg + 1) * shard)
        lse_out[seg] = exchange_blocks(jnp.transpose(cls_lse[span])[:head_count])[:, None, :]
        for off in offsets:
            dest = (sp + off) % sp_size
            remote(
                lse_out.at[seg, dest], ret_lse.at[seg, sp], lback_send.at[seg], lback_recv.at[seg],
                sp=dest,
            ).start()
        ret_lse[seg, sp] = lse_out[seg, sp]
        waits.append(back_total(seg))
        waits.append(lback_total(seg))

    head_lane = lax.broadcasted_iota(jnp.int32, (head_count, PAIR), 1)

    head_row = lax.broadcasted_iota(jnp.int32, (head_count, PAIR), 0)

    def exchange_blocks(x):
        out = x
        for k in range(1, head_count):
            moved = pltpu.roll(pltpu.roll(x, k * share, 1), head_count - k, 0)
            out = jnp.where(head_lane // share == (head_row + k) % head_count, moved, out)
        return out

    def gather_rows(ref, seg):
        return jnp.concatenate([ref[pl.ds(row_of(s, a, c), c)] for s, a, c in spans[seg]], axis=0)

    def combine(seg):
        lback_total(seg).wait_recv()
        flat = exchange_blocks(ret_lse[seg][:, 0, :])
        tall = jnp.transpose(
            jnp.concatenate([flat, jnp.zeros((PAIR - head_count, PAIR), f32)], axis=0)
        )
        for r in range(sp_size):
            lse_f[pl.ds(r, share, stride=sp_size), :] = tall[r * share : (r + 1) * share]
        back_total(seg).wait_recv()
        for g in range(group_count):
            for r in range(sp_size):
                ret_f[g, pl.ds(r, share, stride=sp_size), :] = ret[
                    seg, r * share : (r + 1) * share, g * PAIR : (g + 1) * PAIR
                ].astype(f32)
        la = gather_rows(lse_near, seg)
        lb = lse_f[...]
        peak = jnp.maximum(la, lb)
        ea = jnp.exp(la - peak)
        eb = jnp.exp(lb - peak)
        total = ea + eb
        logw = jnp.transpose(peak + jnp.log(total))[:head_count]
        if seg < 2:
            logw_ref[:, pl.ds(row_of(*spans[seg][0]), shard)] = logw
        else:
            logw_far[seg - 2] = logw
        ea = ea / total
        eb = eb / total
        for g in range(group_count):
            wa = jnp.where(first_head, ea[:, 2 * g : 2 * g + 1], ea[:, 2 * g + 1 : 2 * g + 2])
            wb = jnp.where(first_head, eb[:, 2 * g : 2 * g + 1], eb[:, 2 * g + 1 : 2 * g + 2])
            mixed = wa * gather_rows(o_near.at[g], seg) + wb * ret_f[g]
            att[seg, :, g * PAIR : (g + 1) * PAIR] = mixed.astype(bf16)

    width = wo.shape[1] // OUT_SPLITS

    def product(seg, n):
        return jnp.dot(
            att[seg], wo[:, n * width : (n + 1) * width], preferred_element_type=f32
        ).astype(bf16)

    exch, cross = {}, {}

    def relay(k, n):
        exch[k, n].wait_recv()
        cross_out[k, n] = (keep_b[k, n].astype(f32) + part_in[k, n].astype(f32)).astype(bf16)
        cross[k, n] = remote(
            cross_out.at[k, n], cross_in.at[k, n], cr_send.at[k], cr_recv.at[k, n], tp=far_same
        )
        cross[k, n].start()

    def out_far(k, chunks):
        for n in chunks:
            both = product(2 + k, n)
            part_out[k, n] = both[piece:]
            exch[k, n] = remote(
                part_out.at[k, n], part_in.at[k, n], ex_send.at[k], ex_recv.at[k, n], tp=partner
            )
            exch[k, n].start()
            keep_b[k, n] = both[:piece]
            if n != chunks[0]:
                relay(k, n - 1)
        relay(k, chunks[-1])
        if chunks[-1] == OUT_SPLITS - 1:
            waits.append(bulk(part_out.at[k], ex_send.at[k], ex_recv.at[k, 0]))
            waits.append(bulk(cross_out.at[k], cr_send.at[k], cr_recv.at[k, 0]))

    lse_near[...] = jnp.zeros_like(lse_near)
    cls_lse[...] = jnp.zeros_like(cls_lse)
    halo_early.wait_recv()
    near((far_same, far_other))
    all_groups = range(group_count)
    low_groups, high_groups = all_groups[: group_count // 2], all_groups[group_count // 2 :]
    gathered(0, 1, 4)
    class_lead(2)
    all_groups = range(group_count)
    low_groups, high_groups = all_groups[: group_count // 2], all_groups[group_count // 2 :]
    gathered(5)
    class_rest(2, low_groups)
    send_back(2, low_groups)
    class_rest(2, high_groups)
    send_back(2, high_groups)
    send_sums(2)
    gathered(3)
    class_attend(1)
    scatter(6)
    load_out.wait()
    combine(2)
    halo_late = edge(1 - chip, 1)
    all_chunks = range(OUT_SPLITS)
    out_far(0, all_chunks[: OUT_SPLITS // 2])
    gathered(6)
    class_attend(3, low_groups)
    send_back(3, low_groups)
    class_attend(3, high_groups)
    send_back(3, high_groups)
    send_sums(3)
    out_far(0, all_chunks[OUT_SPLITS // 2 :])
    scatter(2)
    halo_late.wait_recv()
    near((tp, partner))
    combine(3)
    send_back(1, all_groups)
    send_sums(1)
    out_far(1, all_chunks)
    gathered(2)
    class_attend(0)
    send_back(0, all_groups)
    send_sums(0)
    first_half = head_lane < piece
    swap = [pltpu.roll(logw_far[k], piece, 1) for k in range(SPLITS)]
    logw_ref[:, pl.ds(row_of(far_same, 0, shard), shard)] = jnp.where(
        first_half, logw_far[0], swap[1]
    )
    logw_ref[:, pl.ds(row_of(far_other, 0, shard), shard)] = jnp.where(
        first_half, swap[0], logw_far[1]
    )
    combine(1)
    for n in range(OUT_SPLITS):
        own_out[n] = product(1, n)
        remote(own_out.at[n], own_in.at[n], ox_send.at[0], ox_recv.at[0], tp=partner).start()
    own_total = bulk(own_in, ox_send.at[0], ox_recv.at[0])
    waits.append(own_total)
    combine(0)
    for n in range(OUT_SPLITS):
        keep_d[n] = product(0, n).astype(f32)
    own_total.wait_recv()
    for n in range(OUT_SPLITS):
        keep_d[n] = keep_d[n] + own_in[n].astype(f32)
    for k in range(SPLITS):
        for n in range(OUT_SPLITS):
            cross[k, n].wait_recv()
            out_ref[k * piece : (k + 1) * piece, n * width : (n + 1) * width] = (
                keep_d[n, k * piece : (k + 1) * piece] + cross_in[k, n].astype(f32)
            ).astype(bf16)

    for item in waits:
        item.wait_send()


def fused(sp_size, tp_size, tokens_in, w_query, w_key, w_value, w_out):
    shard, depth = tokens_in.shape
    col_count = w_query.shape[1]
    rows = shard * tp_size
    groups = col_count // PAIR
    heads = col_count // HEAD_DIM
    share = shard // sp_size
    piece = shard // SPLITS
    wide = w_out.shape[1]
    width = wide // OUT_SPLITS
    half = HEAD_DIM // 2
    freq = 1.0 / ROTARY_BASE ** (np.arange(half) / half)
    freq = np.tile(freq, PAIR // half)
    start = np.concatenate([np.arange(rows), np.arange(sp_size) * rows])
    angle = start[:, None] * freq[None, :]
    cosine, sine = np.cos(angle), np.sin(angle)
    table = jnp.asarray(np.stack([cosine, sine, cosine, sine]).astype(np.float32))
    f32, bf16 = jnp.float32, jnp.bfloat16
    V_, DMA = pltpu.VMEM, pltpu.SemaphoreType.DMA
    window = ROW_BLOCK + 2 * SIDE_SPAN
    scratch = [
        V_((tp_size, shard, depth), bf16),
        V_((3, depth, col_count), bf16),
        V_((col_count, wide), bf16),
        V_((2,) + table.shape[1:], f32),
        V_((rows, PAIR), f32),
        V_((rows, PAIR), f32),
        V_((rows, col_count), bf16),
        V_((rows + 2 * SIDE_SPAN, 2 * col_count), bf16),
        V_((3 * groups, rows, PAIR), f32),
        V_((sp_size, SEGMENTS * share, 3 * col_count), bf16),
        V_((rows, 3 * col_count), bf16),
        V_((rows, window), f32),
        V_((rows, rows), f32),
        V_((groups, rows, PAIR), f32),
        V_((rows, PAIR), f32),
        V_((rows, col_count), bf16),
        V_((rows, PAIR), f32),
        V_((SEGMENTS, sp_size, 1, PAIR), f32),
        V_((SEGMENTS, shard, col_count), bf16),
        V_((SEGMENTS, sp_size, 1, PAIR), f32),
        V_((groups, shard, PAIR), f32),
        V_((shard, PAIR), f32),
        V_((SPLITS, heads, PAIR), f32),
        V_((groups, shard, PAIR), f32),
        V_((heads, shard, PAIR), f32),
        V_((heads, shard, PAIR), f32),
        V_((SEGMENTS, shard, col_count), bf16),
        V_((SPLITS, OUT_SPLITS, piece, width), bf16),
        V_((SPLITS, OUT_SPLITS, piece, width), bf16),
        V_((SPLITS, OUT_SPLITS, piece, width), bf16),
        V_((SPLITS, OUT_SPLITS, piece, width), bf16),
        V_((SPLITS, OUT_SPLITS, piece, width), bf16),
        V_((OUT_SPLITS, shard, width), f32),
        V_((OUT_SPLITS, shard, width), bf16),
        V_((OUT_SPLITS, shard, width), bf16),
        DMA((6,)),
        DMA((1,)), DMA((1,)),
        DMA((SPLITS,)), DMA((SPLITS,)),
        DMA((SPLITS,)), DMA((SPLITS,)),
        DMA((len(UNITS),)), DMA((len(UNITS),)),
        DMA((2,)), DMA((2,)),
        DMA((SEGMENTS,)), DMA((SEGMENTS,)),
        DMA((SEGMENTS,)), DMA((SEGMENTS,)),
        DMA((SPLITS,)), DMA((SPLITS, OUT_SPLITS)),
        DMA((SPLITS,)), DMA((SPLITS, OUT_SPLITS)),
        DMA((1,)), DMA((1,)),
    ]
    hbm = pl.BlockSpec(memory_space=pltpu.HBM)
    vmem = pl.BlockSpec(memory_space=pltpu.VMEM)
    return pl.pallas_call(
        functools.partial(class_kernel, sp_size, tp_size, col_count),
        out_shape=(
            jax.ShapeDtypeStruct((shard, wide), bf16),
            jax.ShapeDtypeStruct((heads, rows), f32),
        ),
        in_specs=[hbm] * 6,
        out_specs=(vmem, vmem),
        scratch_shapes=scratch,
        compiler_params=pltpu.CompilerParams(
            collective_id=0, has_side_effects=True, vmem_limit_bytes=VMEM_GRANT
        ),
        name="dilated_layer",
    )(tokens_in, w_query, w_key, w_value, w_out, table)


VMEM_GRANT = 52 * 1024 * 1024


def solution(mesh):
    in_specs = (P(("sp", "tp"), None), P(None, "tp"), P(None, "tp"), P(None, "tp"), P("tp", None))
    out_specs = (P(("sp", "tp"), None), P("tp", "sp"))
    sp_size, tp_size = mesh.shape["sp"], mesh.shape["tp"]

    def body(*args):
        shard = args[0].shape[0]
        whole_class = (
            MIDDLE_DILATION % sp_size == 0
            and WIDEST_DILATION % sp_size == 0
            and tp_size == 2 * SPLITS
            and shard == ROW_BLOCK
            and shard == 16 * sp_size
            and args[1].shape[1] == sp_size * HEAD_DIM
        )
        if whole_class:
            return fused(sp_size, tp_size, *args)
        return per_device(*args)

    return jax.shard_map(body, mesh=mesh, in_specs=in_specs, out_specs=out_specs, check_vma=False)
```
